512 devices in a mesh: ep: 32 (over z, core), tp: 16 (over y, x).
Axes of the slice: x: 4, y: 4, z: 16, core: 2. Of those that a mesh axis runs over, the one named last changes fastest.
Arguments:
- gate_out: bfloat16 [8192, 1024], P('ep', 'tp'), may hold values from -6 to 6
- gate_in: bfloat16 [8192, 1024], P('ep', 'tp'), may hold values from -6 to 6
- conv_values: bfloat16 [8192, 1024], P('ep', 'tp'), may hold values from -6 to 6
- conv_taps: float32 [3, 1024], P(None, 'tp'), may hold values from -3 to 3
- mixer_proj: bfloat16 [1024, 2048], P('tp'), may hold values from -0.25 to 0.25
- expert_in: bfloat16 [8192, 2048], P('ep'), may hold values from -6 to 6
- norm_gain: float32 [2048], replicated, may hold values from 0.1 to 1.9
- route_ids: int32 [8192, 2], P('ep'), may hold values from 0 to 31, all different within a row; in each aligned block of 256 rows (0 to 255, 256 to 511, ...) at most 22 rows name the same one
- route_scores: float32 [8192, 2], P('ep'), may hold values from 0.1 to 1
- gate_proj: bfloat16 [32, 2048, 4096], P('ep', None, 'tp'), may hold values from -0.125 to 0.125
- up_proj: bfloat16 [32, 2048, 4096], P('ep', None, 'tp'), may hold values from -0.125 to 0.125
- down_proj: bfloat16 [32, 4096, 2048], P('ep', 'tp'), may hold values from -0.125 to 0.125
Outputs:
- mixed: bfloat16 [8192, 2048], P('ep', 'tp')
- expert_mix: bfloat16 [8192, 2048], P('ep', 'tp')
The draws below stay inside these ranges and needn't reach their ends.
Inputs may be any that keep to these rules, and one draw needn't show every extreme that they name: `route_ids`: each row names 2 different experts. Within each aligned block of 256 rows (the rows of one device of ep) no expert is named by more than 22 rows, and in some block an expert is named by exactly 22 rows.
All inputs are finite; a program needn't handle non-finite values.
Results may differ from the reference program's by a relative error of at most 0.015.
Values may be sent and summed in bfloat16 or wider, within the bound.
No kernel may reach another device: no remote copies, remote signals or barrier semaphores. Data moves between devices by JAX's collectives and lax.ppermute only.
A program may use at most 64 MiB of HBM per device.

```python
import math
from functools import partial
import jax
import jax.numpy as jnp
import numpy as np
from jax import lax

D = 2048
CW = 1024
FF = 4096
KCONV = 3
TOPK = 2
TOKB_EP = 256
EXPERTS = 32
CAP = 22
TOKA = 8192
TOKB = 8192
N_EP = 32
N_TP = 16


def with_spikes(values, rng, source, target, parts, factor):
    owner, partner = [(jnp.arange(values.shape[position]) // (values.shape[position] // parts)).reshape([-1 if axis == position else 1 for axis in range(values.ndim)]) for position in (source, target)]
    chosen = jax.random.permutation(rng, parts)[partner]
    strong = (owner == chosen) | (owner == (partner + parts // 2) % parts)
    return jnp.where(strong, factor * values, values)


def block_scale(key, extent, shards, low, largest):
    gain, own = 1.0, jax.random.fold_in(key, 6)
    for position, parts in shards:
        draws = jnp.exp(jax.random.uniform(jax.random.fold_in(own, position), (parts,), jnp.float32, low / len(shards), largest / len(shards)))
        gain = gain * jnp.repeat(draws, extent[position] // parts).reshape([-1 if axis == position else 1 for axis in range(len(extent))])
    return gain


def deal_out(own_key, own, number, rows, amount, top, bound, skew):
    sequence = jax.random.permutation(own_key, amount)
    heavy_load, usual = shares(amount, rows * top, bound, skew, True), shares(amount, rows * top, bound, skew, False)
    places = jnp.arange(amount)

    def named(tallies, rotation):
        used = int((tallies > 0).sum())
        fixed = max(1, used // 4)
        moved = fixed + (places - fixed + rotation * (used - fixed)) % max(1, amount - fixed)
        return jnp.zeros((amount,), jnp.int32).at[sequence[jnp.where(places < fixed, places, moved)]].set(jnp.asarray(tallies, jnp.int32))

    tallies = jnp.where(number % 4 == 0, named(heavy_load, number // 4), named(usual, number - number // 4 - 1))
    mixed = jax.random.permutation(jax.random.fold_in(own, 3), amount)
    giver, taker = mixed[0:amount // 2 * 2:2], mixed[1:amount // 2 * 2:2]
    room = jnp.minimum(tallies[giver] - 1, bound - tallies[taker]) // 2
    room = jnp.where((giver == sequence[0]) | (taker == sequence[0]) | (tallies[taker] == 0), 0, jnp.maximum(room, 0))
    moved = jax.random.randint(jax.random.fold_in(own, 4), (amount // 2,), 0, 1 << 20) % (room + 1)
    tallies = tallies.at[giver].add(-moved).at[taker].add(moved)
    items = jnp.searchsorted(jnp.cumsum(tallies), jnp.arange(rows * top), side="right").astype(jnp.int32)
    grid = items.reshape(top, rows).T
    grid = grid[jax.random.permutation(jax.random.fold_in(own, 1), rows)]
    rotation = jax.random.randint(jax.random.fold_in(own, 2), (rows, 1), 0, top)
    return jnp.take_along_axis(grid, (jnp.arange(top)[None, :] + rotation) % top, axis=1)


def shares(count, total, reach, skew, full):
    weights = [(1 << 20) // math.isqrt(standing ** skew) + 1 for standing in range(1, count + 1)]
    largest = reach if full else min(reach, max(-(-total // count), total * weights[0] // sum(weights)))
    least = 1 if total - largest >= count - 1 else 0
    holding, rest = [largest] + [least] * (count - 1), total - largest - least * (count - 1)
    while rest > 0:
        free = [i for i in range(1, count) if holding[i] < largest] or [i for i in range(1, count) if holding[i] < reach]
        pool, budget = sum([weights[i] for i in free]), rest
        for i in free:
            extra = min(reach - holding[i], max(1, budget * weights[i] // pool), rest)
            holding[i] = holding[i] + extra
            rest = rest - extra
    return np.array(holding)


def centred(rng, dims, width, most, shards=(), held_as=jnp.bfloat16):
    drawn = width * jax.random.normal(rng, dims, jnp.float32)
    if shards:
        drawn = drawn * block_scale(rng, dims, shards, -0.22, 0.18)
    return jnp.clip(drawn, -most, most).astype(held_as)


def noise_with(key, extent, scale, limit, pieces, heavy, held_as=jnp.bfloat16):
    drawn = scale * jax.random.normal(key, extent, jnp.float32)
    if pieces:
        drawn = drawn * block_scale(key, extent, pieces, -0.22, 0.18)
    return jnp.clip(with_spikes(drawn, jax.random.fold_in(key, 3), *heavy), -limit, limit).astype(held_as)


def setup_inputs(seed: int = 0) -> dict:
    arg_keys = jax.random.split(jax.random.key(seed), 13)
    gate_out = centred(arg_keys[0], (TOKA, CW), 1.0, 6.0, ((0, 32), (1, 16)))
    gate_in = centred(arg_keys[1], (TOKA, CW), 1.0, 6.0, ((0, 32), (1, 16)))
    conv_values = centred(arg_keys[2], (TOKA, CW), 1.0, 6.0, ((0, 32), (1, 16)))
    conv_taps = centred(arg_keys[3], (KCONV, CW), 0.6, 3.0, ((1, 16),), jnp.float32)
    mixer_proj = noise_with(arg_keys[4], (CW, D), CW ** -0.5, 0.25, ((0, 16),), (0, 1, 16, 2.0))
    expert_in = centred(arg_keys[5], (TOKB, D), 1.0, 6.0, ((0, 32),))
    norm_gain = jnp.clip(1.0 + 0.18 * jax.random.normal(arg_keys[6], (D,), jnp.float32), 0.1, 1.9)
    route_ids_keys = jax.random.split(jax.random.fold_in(arg_keys[7], 1), TOKB // TOKB_EP)
    route_ids_turns = jax.random.permutation(jax.random.fold_in(arg_keys[7], 3), TOKB // TOKB_EP)
    route_ids = jax.vmap(lambda own, number: deal_out(jax.random.fold_in(arg_keys[7], 2), own, number, TOKB_EP, EXPERTS, TOPK, CAP, 1))(route_ids_keys, route_ids_turns).reshape((TOKB, TOPK))
    route_scores = jnp.clip(0.1 + 0.9 * jax.random.uniform(arg_keys[8], (TOKB, TOPK), jnp.float32) ** block_scale(arg_keys[8], (TOKB, TOPK), ((0, 32),), -0.2, 0.2), 0.1, 1.0)
    gate_proj = centred(arg_keys[9], (EXPERTS, D, FF), D ** -0.5, 0.125, ((0, 32), (2, 16)))
    up_proj = centred(arg_keys[10], (EXPERTS, D, FF), D ** -0.5, 0.125, ((0, 32), (2, 16)))
    down_proj = noise_with(arg_keys[11], (EXPERTS, FF, D), FF ** -0.5, 0.125, ((0, 32), (1, 16)), (1, 2, 16, 2.0))
    return {"gate_out": gate_out, "gate_in": gate_in, "conv_values": conv_values, "conv_taps": conv_taps, "mixer_proj": mixer_proj, "expert_in": expert_in, "norm_gain": norm_gain, "route_ids": route_ids, "route_scores": route_scores, "gate_proj": gate_proj, "up_proj": up_proj, "down_proj": down_proj}


def slot_table(route_ids, experts_total, capacity):
    pairs = route_ids.reshape(-1)
    onehot = (pairs[:, None] == jnp.arange(experts_total, dtype=jnp.int32)[None, :]).astype(jnp.int32)
    before = jnp.cumsum(onehot, axis=0) - onehot
    ranking = lax.optimization_barrier(jnp.sum(before * onehot, axis=1))
    return (pairs * capacity + ranking).astype(jnp.int32).reshape(route_ids.shape)

def block_sum(left, right, blocks):
    row_count = left.shape[0]
    inner_width = left.shape[1] // blocks
    left_blocks = left.reshape(row_count, blocks, inner_width).transpose(1, 0, 2)
    right_blocks = right.reshape(blocks, inner_width, right.shape[1])

    def add_block(running, operands):
        rounded = jnp.dot(operands[0], operands[1], preferred_element_type=jnp.float32).astype(jnp.bfloat16)
        rounded = lax.optimization_barrier(rounded)
        return (running + rounded.astype(jnp.float32), None)
    start_sum = jnp.zeros((row_count, right.shape[1]), jnp.float32)
    running, _ = lax.scan(add_block, start_sum, (left_blocks, right_blocks))
    return running

def pick_rows(table, index):
    return jnp.take(table, index, axis=0)

def run_expert(operands):
    tokens, w_gate, w_up, w_down = operands
    gate_value = jnp.dot(tokens, w_gate, preferred_element_type=jnp.float32)
    up_value = jnp.dot(tokens, w_up, preferred_element_type=jnp.float32)
    hidden = (jax.nn.silu(gate_value) * up_value).astype(jnp.bfloat16)
    return block_sum(hidden, w_down, N_TP).astype(jnp.bfloat16)

def reference(gate_out, gate_in, conv_values, conv_taps, mixer_proj, expert_in, norm_gain, route_ids, route_scores, gate_proj, up_proj, down_proj):
    product = gate_in.astype(jnp.float32) * conv_values.astype(jnp.float32)
    seq_len = product.shape[0]
    padded = jnp.concatenate([jnp.zeros((KCONV - 1, CW), jnp.float32), product], axis=0)
    convolved = conv_taps[0] * padded[0:seq_len]
    for offset in range(1, KCONV):
        convolved = convolved + conv_taps[offset] * padded[offset:offset + seq_len]
    branch = (gate_out.astype(jnp.float32) * convolved).astype(jnp.bfloat16)
    mixed = block_sum(branch, mixer_proj, N_TP).astype(jnp.bfloat16)
    rows_wide = expert_in.astype(jnp.float32)
    scaling = lax.rsqrt(lax.optimization_barrier(jnp.mean(rows_wide * rows_wide, axis=1, keepdims=True)) + 1e-06)
    normed = (rows_wide * scaling * norm_gain).astype(jnp.bfloat16)
    slot_count = EXPERTS * CAP
    route_blocks = route_ids.reshape(N_EP, TOKB_EP, TOPK)
    slots = jax.vmap(partial(slot_table, experts_total=EXPERTS, capacity=CAP))(route_blocks)
    sources = jnp.arange(N_EP, dtype=jnp.int32)[:, None, None] * jnp.ones_like(slots)
    token_index = jnp.arange(TOKB_EP, dtype=jnp.int32)[None, :, None] * jnp.ones_like(slots)
    owner = jnp.full((N_EP, slot_count), TOKB_EP, jnp.int32)
    owner = owner.at[sources.reshape(-1), slots.reshape(-1)].set(token_index.reshape(-1))
    normed_blocks = normed.reshape(N_EP, TOKB_EP, D)
    padded_rows = jnp.concatenate([normed_blocks, jnp.zeros((N_EP, 1, D), jnp.bfloat16)], axis=1)
    buffer = jax.vmap(pick_rows)(padded_rows, owner)
    by_expert = buffer.reshape(N_EP, EXPERTS, CAP, D).transpose(1, 0, 2, 3).reshape(EXPERTS, N_EP * CAP, D)
    outputs = lax.map(run_expert, (by_expert, gate_proj, up_proj, down_proj))
    results = outputs.reshape(EXPERTS, N_EP, CAP, D)
    positions = (slots - route_blocks * CAP).astype(jnp.int32)
    picked = results[route_blocks, sources, positions].astype(jnp.float32)
    weights = route_scores / lax.optimization_barrier(jnp.sum(route_scores, axis=1, keepdims=True))
    weights = weights.reshape(N_EP, TOKB_EP, TOPK)
    expert_mix = lax.optimization_barrier(jnp.sum(weights[:, :, :, None] * picked, axis=2)).astype(jnp.bfloat16).reshape(TOKB, D)
    return (mixed, expert_mix)
```

```python
import jax
import jax.numpy as jnp
from jax import lax
from jax.experimental import pallas as pl
from jax.experimental.pallas import tpu as pltpu
from jax.sharding import Mesh
from jax.sharding import PartitionSpec as P

TP = ("tp_0", "tp_1")
F32 = jnp.float32
BF16 = jnp.bfloat16
VMEM = pl.BlockSpec(memory_space=pltpu.VMEM)
SMEM = pl.BlockSpec(memory_space=pltpu.SMEM)


def shifted(block, axis, distance):
    devices = range(lax.axis_size(axis))
    route = [(i - distance, i) for i in devices if i - distance in devices]
    return lax.ppermute(block, axis, route)


def call(body, out, limit, flops, *operands, specs=None):
    return pl.pallas_call(
        body,
        out_shape=out,
        in_specs=specs or [VMEM] * len(operands),
        out_specs=jax.tree.map(lambda _: VMEM, out),
        compiler_params=pltpu.CompilerParams(vmem_limit_bytes=limit),
        cost_estimate=pl.CostEstimate(
            flops=flops, bytes_accessed=1 << 20, transcendentals=0
        ),
    )(*operands)


def dispatch_body(capacity, experts, place, rows, gain, ids, sent, slots):
    tokens, width = rows.shape
    columns = sent.shape[1]
    wide = rows[...].astype(F32)
    scaling = lax.rsqrt(jnp.sum(wide * wide, axis=1, keepdims=True) / width + 1e-06)
    start = pl.multiple_of(place[0] * columns, columns)
    own = rows[:, pl.ds(start, columns)].astype(F32)
    normed = (own * scaling * gain[:, pl.ds(start, columns)]).astype(BF16)
    chosen = ids[...]
    expert = lax.broadcasted_iota(jnp.int32, (experts, tokens), 0)
    hits = [expert == chosen[k : k + 1, :] for k in range(chosen.shape[0])]
    marks = [jnp.where(h, 1.0, 0.0).astype(F32) for h in hits]
    total = marks[0]
    for m in marks[1:]:
        total = total + m
    earlier = lax.broadcasted_iota(jnp.int32, (tokens, tokens), 0)
    later = lax.broadcasted_iota(jnp.int32, (tokens, tokens), 1)
    before = jnp.dot(
        total.astype(BF16),
        jnp.where(earlier < later, 1.0, 0.0).astype(BF16),
        preferred_element_type=F32,
    )
    base = (expert * capacity).astype(F32)
    where = [
        jnp.sum(m * (before + base), axis=0, keepdims=True).astype(jnp.int32) for m in marks
    ]
    slots[...] = jnp.concatenate(where, axis=0)
    slot = lax.broadcasted_iota(jnp.int32, (sent.shape[0], tokens), 0)
    table = slot == where[0]
    for w in where[1:]:
        table = table | (slot == w)
    sent[...] = jnp.dot(
        jnp.where(table, 1.0, 0.0).astype(BF16), normed, preferred_element_type=F32
    ).astype(BF16)


def expert_body(step, tokens, gate_w, up_w, down_w, branch, mixer_w, out):
    blocks, rows, columns = tokens.shape

    def tile(number, carry):
        at = pl.ds(pl.multiple_of(number * step, step), step)
        left = jnp.concatenate([tokens[b, at, :] for b in range(blocks)], axis=1)
        gate = jnp.dot(left, gate_w[...], preferred_element_type=F32)
        up = jnp.dot(left, up_w[...], preferred_element_type=F32)
        hidden = (gate / (1.0 + jnp.exp(-gate)) * up).astype(BF16)
        part = jnp.dot(hidden, down_w[...], preferred_element_type=F32).astype(BF16)
        for b in range(blocks):
            out[b, at, :] = part[:, b * columns : (b + 1) * columns]
        return carry

    lax.fori_loop(0, rows // step, tile, 0)
    part = jnp.dot(branch[...], mixer_w[...], preferred_element_type=F32).astype(BF16)
    for b in range(blocks):
        out[b, rows:, :] = part[:, b * columns : (b + 1) * columns]


def total_body(parts, outputs, mixed):
    rows = outputs.shape[0]
    total = parts[0].astype(F32)
    for b in range(1, parts.shape[0]):
        total = total + parts[b].astype(F32)
    total = total.astype(BF16)
    outputs[...] = total[:rows]
    mixed[...] = total[rows:]


def combine_body(rows, slots, scores, out):
    tokens = out.shape[0]
    slot = lax.broadcasted_iota(jnp.int32, (tokens, rows.shape[0]), 1)
    held = rows[...]
    score = scores[...]
    whole = jnp.sum(score, axis=1, keepdims=True)
    total = None
    for k in range(score.shape[1]):
        pick = jnp.where(slot == slots[:, k : k + 1], 1.0, 0.0).astype(BF16)
        term = jnp.dot(pick, held, preferred_element_type=F32)
        term = term * (score[:, k : k + 1] / whole)
        total = term if total is None else total + term
    out[...] = total.astype(BF16)


def shards(
    gate_out,
    gate_in,
    conv_values,
    conv_taps,
    mixer_proj,
    expert_in,
    norm_gain,
    route_ids,
    route_scores,
    gate_proj,
    up_proj,
    down_proj,
):
    tokens, choices = route_ids.shape
    width = expert_in.shape[1]
    ep_count = lax.axis_size("ep")
    tp_count = lax.axis_size(TP)
    local_experts = gate_proj.shape[0]
    experts = ep_count * local_experts
    capacity = max(2, (4 * tokens * choices + 3 * experts - 1) // (3 * experts))
    slot_count = experts * capacity
    columns = width // tp_count
    place = lax.axis_index(TP).astype(jnp.int32).reshape(1)

    sent, slots = call(
        lambda *refs: dispatch_body(capacity, experts, *refs),
        (
            jax.ShapeDtypeStruct((slot_count, columns), BF16),
            jax.ShapeDtypeStruct((choices, tokens), jnp.int32),
        ),
        16 << 20,
        1 << 28,
        place,
        expert_in,
        norm_gain.reshape(1, width),
        route_ids.T,
        specs=[SMEM, VMEM, VMEM, VMEM],
    )
    arrived = lax.all_to_all(
        sent.reshape(experts, capacity, columns), "ep", split_axis=0, concat_axis=0, tiled=True
    )
    own_block = arrived.reshape(1, slot_count, columns)
    copies = jnp.broadcast_to(own_block, (tp_count, slot_count, columns))
    gathered = lax.all_to_all(copies, TP, 0, 0, tiled=True)

    product = gate_in.astype(F32) * conv_values.astype(F32)
    seq_len = product.shape[0]
    tap_count = conv_taps.shape[0]
    earlier = shifted(product[seq_len - (tap_count - 1) :], "ep", 1)
    padded = jnp.concatenate([earlier, product], axis=0)
    convolved = conv_taps[0] * padded[0:seq_len]
    for offset in range(1, tap_count):
        convolved = convolved + conv_taps[offset] * padded[offset : offset + seq_len]
    branch = (gate_out.astype(F32) * convolved).astype(BF16)

    step = slot_count // 4
    parts = call(
        lambda *refs: expert_body(step, *refs),
        jax.ShapeDtypeStruct((tp_count, slot_count + seq_len, columns), BF16),
        24 << 20,
        1 << 32,
        gathered,
        gate_proj[0],
        up_proj[0],
        down_proj[0],
        branch,
        mixer_proj,
    )
    shared = lax.all_to_all(parts, TP, 0, 0, tiled=True)
    outputs, mixed = call(
        total_body,
        (
            jax.ShapeDtypeStruct((slot_count, columns), BF16),
            jax.ShapeDtypeStruct((seq_len, columns), BF16),
        ),
        16 << 20,
        1 << 24,
        shared,
    )
    returned = lax.all_to_all(
        outputs.reshape(experts, capacity, columns), "ep", split_axis=0, concat_axis=0, tiled=True
    )
    expert_mix = call(
        combine_body,
        jax.ShapeDtypeStruct((tokens, columns), BF16),
        16 << 20,
        1 << 27,
        returned.reshape(slot_count, columns),
        slots.T,
        route_scores,
    )
    return (mixed, expert_mix)


def solution(mesh):
    torus = Mesh(mesh.devices.reshape(mesh.shape["ep"], 4, 4), ("ep", "tp_0", "tp_1"))
    in_specs = (
        P("ep", TP),
        P("ep", TP),
        P("ep", TP),
        P(None, TP),
        P(TP, None),
        P("ep", None),
        P(),
        P("ep", None),
        P("ep", None),
        P("ep", None, TP),
        P("ep", None, TP),
        P("ep", TP, None),
    )
    out_specs = (P("ep", TP), P("ep", TP))
    return jax.shard_map(
        shards, mesh=torus, in_specs=in_specs, out_specs=out_specs, check_vma=False
    )
```

```python
import jax
import jax.numpy as jnp
from jax import lax
from jax.experimental import pallas as pl
from jax.experimental.pallas import tpu as pltpu
from jax.sharding import Mesh
from jax.sharding import PartitionSpec as P


TP = ("tp_0", "tp_1")
F32 = jnp.float32
BF16 = jnp.bfloat16
VMEM = pl.BlockSpec(memory_space=pltpu.VMEM)
SMEM = pl.BlockSpec(memory_space=pltpu.SMEM)
HBM = pl.BlockSpec(memory_space=pltpu.HBM)


def shifted(block, axis, distance):
    devices = range(lax.axis_size(axis))
    route = [(i - distance, i) for i in devices if i - distance in devices]
    return lax.ppermute(block, axis, route)


def call(body, out, limit, flops, *operands, specs=None, scratch=()):
    return pl.pallas_call(
        body,
        out_shape=out,
        in_specs=specs or [VMEM] * len(operands),
        out_specs=jax.tree.map(lambda _: VMEM, out),
        scratch_shapes=scratch,
        compiler_params=pltpu.CompilerParams(vmem_limit_bytes=limit),
        cost_estimate=pl.CostEstimate(
            flops=flops, bytes_accessed=1 << 20, transcendentals=0
        ),
    )(*operands)


def dispatch_body(
    stride, experts, place, rows_far, gain_far, ids_far, sent, slots, rows, gain, ids, done
):
    copies = [
        pltpu.make_async_copy(far, near, done.at[n])
        for n, (far, near) in enumerate(((ids_far, ids), (gain_far, gain), (rows_far, rows)))
    ]
    for copy in copies:
        copy.start()
    for copy in copies:
        copy.wait()
    tokens, width = rows.shape
    capacity, columns = sent.shape[1:]
    wide = rows[...].astype(F32)
    scaling = lax.rsqrt(jnp.sum(wide * wide, axis=1, keepdims=True) / width + 1e-06)
    start = pl.multiple_of(place[0] * columns, columns)
    own = rows[:, pl.ds(start, columns)].astype(F32)
    normed = (own * scaling * gain[:, pl.ds(start, columns)]).astype(BF16)
    chosen = ids[...]
    expert = lax.broadcasted_iota(jnp.int32, (experts, tokens), 0)
    hits = [expert == chosen[k : k + 1, :] for k in range(chosen.shape[0])]
    marks = [jnp.where(h, 1.0, 0.0).astype(F32) for h in hits]
    total = marks[0]
    for m in marks[1:]:
        total = total + m
    earlier = lax.broadcasted_iota(jnp.int32, (tokens, tokens), 0)
    later = lax.broadcasted_iota(jnp.int32, (tokens, tokens), 1)
    before = jnp.dot(
        total.astype(BF16),
        jnp.where(earlier < later, 1.0, 0.0).astype(BF16),
        preferred_element_type=F32,
    )
    base = (expert * stride).astype(F32)
    where = [
        jnp.sum(m * (before + base), axis=0, keepdims=True).astype(jnp.int32) for m in marks
    ]
    slots[...] = jnp.concatenate(where, axis=0)
    slot = lax.broadcasted_iota(jnp.int32, (experts * stride, tokens), 0)
    table = slot == where[0]
    for w in where[1:]:
        table = table | (slot == w)
    placed = jnp.dot(
        jnp.where(table, 1.0, 0.0).astype(BF16), normed, preferred_element_type=F32
    ).reshape(experts, stride, columns)
    sent[...] = placed[:, :capacity, :].astype(BF16)


def expert_body(step, tokens, gate_w, up_w, down_w, out):
    blocks, rows, columns = tokens.shape

    def tile(number, carry):
        at = pl.ds(pl.multiple_of(number * step, step), step)
        left = jnp.concatenate([tokens[b, at, :] for b in range(blocks)], axis=1)
        gate = jnp.dot(left, gate_w[0], preferred_element_type=F32)
        up = jnp.dot(left, up_w[0], preferred_element_type=F32)
        hidden = (gate / (1.0 + jnp.exp(-gate)) * up).astype(BF16)
        part = jnp.dot(hidden, down_w[0], preferred_element_type=F32).astype(BF16)
        for b in range(blocks):
            out[b, at, :] = part[:, b * columns : (b + 1) * columns]
        return carry

    lax.fori_loop(0, rows // step, tile, 0)


def sum_body(parts, out, total):
    experts, capacity, _ = out.shape
    value = parts[0].astype(F32)
    for b in range(1, parts.shape[0]):
        value = value + parts[b].astype(F32)
    total[...] = value
    for e in range(experts):
        out[e] = total[e * capacity : (e + 1) * capacity, :].astype(BF16)


def mixer_body(place, gate_out, gate_in, values, taps, halo, proj, *outs):
    count = len(outs)
    groups, _, columns = outs[0].shape
    product = gate_in[...].astype(F32).T * values[...].astype(F32).T
    row = lax.broadcasted_iota(jnp.int32, product.shape, 0)
    last = halo[1:2, :]
    back_one = jnp.where(row == 0, last, pltpu.roll(product, 1, 0))
    back_two = jnp.where(
        row == 0, halo[0:1, :], jnp.where(row == 1, last, pltpu.roll(product, 2, 0))
    )
    convolved = taps[0:1, :] * back_two + taps[1:2, :] * back_one + taps[2:3, :] * product
    branch = (gate_out[...].astype(F32).T * convolved).astype(BF16)
    for away, out in enumerate(outs):
        target = lax.rem(place[0] + away, count)
        for g in range(groups):
            start = pl.multiple_of((g * count + target) * columns, columns)
            out[g] = jnp.dot(
                branch, proj[:, pl.ds(start, columns)], preferred_element_type=F32
            ).astype(BF16)


def regroup_body(place, *refs):
    half = len(refs) // 2
    parts, outs = refs[:half], refs[half:]
    for away, out in enumerate(outs):
        target = lax.rem(place[0] + away, half)
        total = parts[0][target].astype(F32)
        for part in parts[1:]:
            total = total + part[target].astype(F32)
        out[...] = total.astype(BF16)


def final_body(*refs):
    total = refs[0][...].astype(F32)
    for part in refs[1:-1]:
        total = total + part[...].astype(F32)
    refs[-1][...] = total.astype(BF16)


def turned(block, axis, distance):
    count = lax.axis_size(axis)
    return lax.ppermute(block, axis, [(i, (i + distance) % count) for i in range(count)])


def combine_body(rows, slots, scores, out, padded):
    tokens = out.shape[0]
    experts, capacity, columns = rows.shape
    stride = padded.shape[1]
    slot = lax.broadcasted_iota(jnp.int32, (tokens, experts * stride), 1)
    padded[...] = jnp.zeros_like(padded)
    padded[:, :capacity, :] = rows[...].astype(F32)
    held = padded[...].reshape(experts * stride, columns).astype(BF16)
    score = scores[...]
    whole = jnp.sum(score, axis=1, keepdims=True)
    total = None
    for k in range(score.shape[1]):
        pick = jnp.where(slot == slots[:, k : k + 1], 1.0, 0.0).astype(BF16)
        term = jnp.dot(pick, held, preferred_element_type=F32)
        term = term * (score[:, k : k + 1] / whole)
        total = term if total is None else total + term
    out[...] = total.astype(BF16)


def shards(
    gate_out,
    gate_in,
    conv_values,
    conv_taps,
    mixer_proj,
    expert_in,
    norm_gain,
    route_ids,
    route_scores,
    gate_proj,
    up_proj,
    down_proj,
):
    tokens, choices = route_ids.shape
    width = expert_in.shape[1]
    ep_count = lax.axis_size("ep")
    tp_count = lax.axis_size(TP)
    local_experts = gate_proj.shape[0]
    experts = ep_count * local_experts
    capacity = max(2, (4 * tokens * choices + 3 * experts - 1) // (3 * experts))
    slot_count = experts * capacity
    stride = (capacity + 7) // 8 * 8
    columns = width // tp_count
    place = lax.axis_index(TP).astype(jnp.int32).reshape(1)
    place_0 = lax.axis_index(TP[0]).astype(jnp.int32).reshape(1)
    place_1 = lax.axis_index(TP[1]).astype(jnp.int32).reshape(1)
    groups = lax.axis_size(TP[0])
    turns = lax.axis_size(TP[1])
    seq_len = gate_in.shape[0]
    tail = seq_len - (conv_taps.shape[0] - 1)

    halo = shifted(gate_in[tail:].astype(F32) * conv_values[tail:].astype(F32), "ep", 1)

    sent, slots = call(
        lambda *refs: dispatch_body(stride, experts, *refs),
        (
            jax.ShapeDtypeStruct((experts, capacity, columns), BF16),
            jax.ShapeDtypeStruct((choices, tokens), jnp.int32),
        ),
        56 << 20,
        1 << 28,
        place,
        expert_in,
        norm_gain.reshape(1, width),
        route_ids.T,
        specs=[SMEM, HBM, HBM, HBM],
        scratch=[
            pltpu.VMEM((tokens, width), BF16),
            pltpu.VMEM((1, width), F32),
            pltpu.VMEM((choices, tokens), jnp.int32),
            pltpu.SemaphoreType.DMA((3,)),
        ],
    )
    arrived = lax.all_to_all(sent, "ep", 0, 0, tiled=True)

    first = call(
        mixer_body,
        (jax.ShapeDtypeStruct((groups, seq_len, columns), BF16),) * turns,
        56 << 20,
        1 << 26,
        place_1,
        gate_out.T,
        gate_in.T,
        conv_values.T,
        conv_taps,
        halo,
        mixer_proj,
        specs=[SMEM] + [VMEM] * 6,
    )
    first = [first[0]] + [turned(first[d], TP[1], d) for d in range(1, turns)]

    own_block = arrived.reshape(1, slot_count, columns)
    copies = jnp.broadcast_to(own_block, (tp_count, slot_count, columns))
    gathered = lax.all_to_all(copies, TP, 0, 0, tiled=True)
    parts = call(
        lambda *refs: expert_body(slot_count // 4, *refs),
        jax.ShapeDtypeStruct((tp_count, slot_count, columns), BF16),
        24 << 20,
        1 << 32,
        gathered,
        gate_proj,
        up_proj,
        down_proj,
    )
    shared = lax.all_to_all(parts, TP, 0, 0, tiled=True)
    outputs = call(
        sum_body,
        jax.ShapeDtypeStruct((experts, capacity, columns), BF16),
        16 << 20,
        1 << 24,
        shared,
        scratch=[pltpu.VMEM((slot_count, columns), F32)],
    )
    returned = lax.all_to_all(outputs, "ep", 0, 0, tiled=True)

    second = call(
        regroup_body,
        (jax.ShapeDtypeStruct((seq_len, columns), BF16),) * groups,
        12 << 20,
        1 << 22,
        place_0,
        *first,
        specs=[SMEM] + [VMEM] * turns,
    )
    second = [second[0]] + [turned(second[d], TP[0], d) for d in range(1, groups)]
    mixed = call(
        final_body, jax.ShapeDtypeStruct((seq_len, columns), BF16), 8 << 20, 1 << 20, *second
    )
    expert_mix = call(
        combine_body,
        jax.ShapeDtypeStruct((tokens, columns), BF16),
        16 << 20,
        1 << 27,
        returned,
        slots.T,
        route_scores,
        scratch=[pltpu.VMEM((experts, stride, columns), F32)],
    )
    return (mixed, expert_mix)


def solution(mesh):
    torus = Mesh(mesh.devices.reshape(mesh.shape["ep"], 4, 4), ("ep", "tp_0", "tp_1"))
    in_specs = (
        P("ep", TP),
        P("ep", TP),
        P("ep", TP),
        P(None, TP),
        P(TP, None),
        P("ep", None),
        P(),
        P("ep", None),
        P("ep", None),
        P("ep", None, TP),
        P("ep", None, TP),
        P("ep", TP, None),
    )
    out_specs = (P("ep", TP), P("ep", TP))

    return jax.shard_map(
        shards, mesh=torus, in_specs=in_specs, out_specs=out_specs, check_vma=False
    )
```

```python
import jax
import jax.numpy as jnp
from jax import lax
from jax.experimental import pallas as pl
from jax.experimental.pallas import tpu as pltpu
from jax.sharding import Mesh
from jax.sharding import PartitionSpec as P


TP = ("tp_0", "tp_1")
F32 = jnp.float32
BF16 = jnp.bfloat16
VMEM = pl.BlockSpec(memory_space=pltpu.VMEM)
SMEM = pl.BlockSpec(memory_space=pltpu.SMEM)
HBM = pl.BlockSpec(memory_space=pltpu.HBM)


def shifted(block, axis, distance):
    devices = range(lax.axis_size(axis))
    route = [(i - distance, i) for i in devices if i - distance in devices]
    return lax.ppermute(block, axis, route)


def call(body, out, limit, flops, *operands, specs=None, scratch=(), place=None):
    return pl.pallas_call(
        body,
        out_shape=out,
        in_specs=specs or [VMEM] * len(operands),
        out_specs=jax.tree.map(lambda _: place or VMEM, out),
        scratch_shapes=scratch,
        compiler_params=pltpu.CompilerParams(vmem_limit_bytes=limit),
        cost_estimate=pl.CostEstimate(
            flops=flops, bytes_accessed=1 << 20, transcendentals=0
        ),
    )(*operands)


def far(array):
    return pltpu.with_memory_space_constraint(array, pltpu.HBM)


def dispatch_body(
    stride,
    experts,
    place,
    rows_far,
    gain_far,
    ids_far,
    inner_far,
    values_far,
    outer_far,
    proj_far,
    sent,
    slots,
    tail,
    product,
    outer,
    proj,
    rows,
    gain,
    ids,
    inner,
    values,
    done,
):
    pairs = (
        (rows_far, rows),
        (gain_far, gain),
        (ids_far, ids),
        (inner_far, inner),
        (values_far, values),
        (outer_far, outer),
        (proj_far, proj),
    )
    copies = [
        pltpu.make_async_copy(there, here, done.at[n]) for n, (there, here) in enumerate(pairs)
    ]
    for copy in copies:
        copy.start()
    for copy in copies[3:5]:
        copy.wait()
    mixed = inner[...].astype(F32).T * values[...].astype(F32).T
    product[...] = mixed
    tail[...] = mixed[mixed.shape[0] - tail.shape[0] :, :]
    for copy in copies[:3] + copies[5:]:
        copy.wait()
    tokens, width = rows.shape
    capacity, columns = sent.shape[1:]
    wide = rows[...].astype(F32)
    scaling = lax.rsqrt(jnp.sum(wide * wide, axis=1, keepdims=True) / width + 1e-06)
    start = pl.multiple_of(place[0] * columns, columns)
    own = rows[:, pl.ds(start, columns)].astype(F32)
    normed = (own * scaling * gain[:, pl.ds(start, columns)]).astype(BF16)
    chosen = ids[...]
    expert = lax.broadcasted_iota(jnp.int32, (experts, tokens), 0)
    hits = [expert == chosen[k : k + 1, :] for k in range(chosen.shape[0])]
    marks = [jnp.where(h, 1.0, 0.0).astype(F32) for h in hits]
    total = marks[0]
    for m in marks[1:]:
        total = total + m
    earlier = lax.broadcasted_iota(jnp.int32, (tokens, tokens), 0)
    later = lax.broadcasted_iota(jnp.int32, (tokens, tokens), 1)
    before = jnp.dot(
        total.astype(BF16),
        jnp.where(earlier < later, 1.0, 0.0).astype(BF16),
        preferred_element_type=F32,
    )
    base = (expert * stride).astype(F32)
    where = [
        jnp.sum(m * (before + base), axis=0, keepdims=True).astype(jnp.int32) for m in marks
    ]
    slots[...] = jnp.concatenate(where, axis=0)
    slot = lax.broadcasted_iota(jnp.int32, (experts * stride, tokens), 0)
    table = slot == where[0]
    for w in where[1:]:
        table = table | (slot == w)
    placed = jnp.dot(
        jnp.where(table, 1.0, 0.0).astype(BF16), normed, preferred_element_type=F32
    ).reshape(experts, stride, columns)
    sent[...] = placed[:, :capacity, :].astype(BF16)


def expert_body(step, tokens, gate_w, up_w, down_w, out, held, done):
    blocks, rows, columns = tokens.shape
    slots = held.shape[0]
    copies = []
    for number in range(rows // step):
        at = slice(number * step, (number + 1) * step)
        left = jnp.concatenate([tokens[b, at, :] for b in range(blocks)], axis=1)
        gate = jnp.dot(left, gate_w[0], preferred_element_type=F32)
        up = jnp.dot(left, up_w[0], preferred_element_type=F32)
        hidden = (gate / (1.0 + jnp.exp(-gate)) * up).astype(BF16)
        part = jnp.dot(hidden, down_w[0], preferred_element_type=F32).astype(BF16)
        slot = number % slots
        if number >= slots:
            copies[number - slots].wait()
        for b in range(blocks):
            held[slot, b] = part[:, b * columns : (b + 1) * columns]
        copies.append(
            pltpu.make_async_copy(held.at[slot], out.at[:, pl.ds(at.start, step), :], done.at[slot])
        )
        copies[-1].start()
    for copy in copies[-slots:]:
        copy.wait()


def sum_body(parts, out, total):
    experts, capacity, _ = out.shape
    value = parts[0].astype(F32)
    for b in range(1, parts.shape[0]):
        value = value + parts[b].astype(F32)
    total[...] = value
    for e in range(experts):
        out[e] = total[e * capacity : (e + 1) * capacity, :].astype(BF16)


def mixer_body(place, outer, product_ref, taps, halo, proj, *outs):
    count = len(outs)
    groups, _, columns = outs[0].shape
    product = product_ref[...]
    row = lax.broadcasted_iota(jnp.int32, product.shape, 0)
    last = halo[1:2, :]
    back_one = jnp.where(row == 0, last, pltpu.roll(product, 1, 0))
    back_two = jnp.where(
        row == 0, halo[0:1, :], jnp.where(row == 1, last, pltpu.roll(product, 2, 0))
    )
    convolved = taps[0:1, :] * back_two + taps[1:2, :] * back_one + taps[2:3, :] * product
    branch = (outer[...].astype(F32).T * convolved).astype(BF16)
    for away, out in enumerate(outs):
        target = lax.rem(place[0] + away, count)
        for g in range(groups):
            start = pl.multiple_of((g * count + target) * columns, columns)
            out[g] = jnp.dot(
                branch, proj[:, pl.ds(start, columns)], preferred_element_type=F32
            ).astype(BF16)


def regroup_body(place, *refs):
    half = len(refs) // 2
    parts, outs = refs[:half], refs[half:]
    for away, out in enumerate(outs):
        target = lax.rem(place[0] + away, half)
        total = parts[0][target].astype(F32)
        for part in parts[1:]:
            total = total + part[target].astype(F32)
        out[...] = total.astype(BF16)


def final_body(*refs):
    total = refs[0][...].astype(F32)
    for part in refs[1:-1]:
        total = total + part[...].astype(F32)
    refs[-1][...] = total.astype(BF16)


def turned(block, axis, distance):
    count = lax.axis_size(axis)
    return lax.ppermute(block, axis, [(i, (i + distance) % count) for i in range(count)])


def combine_body(rows, slots, scores, out, padded):
    tokens = out.shape[0]
    experts, capacity, columns = rows.shape
    stride = padded.shape[1]
    slot = lax.broadcasted_iota(jnp.int32, (tokens, experts * stride), 1)
    padded[...] = jnp.zeros_like(padded)
    padded[:, :capacity, :] = rows[...].astype(F32)
    held = padded[...].reshape(experts * stride, columns).astype(BF16)
    score = scores[...]
    whole = jnp.sum(score, axis=1, keepdims=True)
    total = None
    for k in range(score.shape[1]):
        pick = jnp.where(slot == slots[:, k : k + 1], 1.0, 0.0).astype(BF16)
        term = jnp.dot(pick, held, preferred_element_type=F32)
        term = term * (score[:, k : k + 1] / whole)
        total = term if total is None else total + term
    out[...] = total.astype(BF16)


def shards(
    gate_out,
    gate_in,
    conv_values,
    conv_taps,
    mixer_proj,
    expert_in,
    norm_gain,
    route_ids,
    route_scores,
    gate_proj,
    up_proj,
    down_proj,
):
    tokens, choices = route_ids.shape
    width = expert_in.shape[1]
    ep_count = lax.axis_size("ep")
    tp_count = lax.axis_size(TP)
    local_experts = gate_proj.shape[0]
    experts = ep_count * local_experts
    capacity = max(2, (4 * tokens * choices + 3 * experts - 1) // (3 * experts))
    slot_count = experts * capacity
    stride = (capacity + 7) // 8 * 8
    columns = width // tp_count
    place = lax.axis_index(TP).astype(jnp.int32).reshape(1)
    place_0 = lax.axis_index(TP[0]).astype(jnp.int32).reshape(1)
    place_1 = lax.axis_index(TP[1]).astype(jnp.int32).reshape(1)
    groups = lax.axis_size(TP[0])
    turns = lax.axis_size(TP[1])
    seq_len = gate_in.shape[0]
    channels = gate_in.shape[1]

    sent, slots, tail, product, outer, proj = call(
        lambda *refs: dispatch_body(stride, experts, *refs),
        (
            jax.ShapeDtypeStruct((experts, capacity, columns), BF16),
            jax.ShapeDtypeStruct((choices, tokens), jnp.int32),
            jax.ShapeDtypeStruct((conv_taps.shape[0] - 1, channels), F32),
            jax.ShapeDtypeStruct((seq_len, channels), F32),
            jax.ShapeDtypeStruct((channels, seq_len), BF16),
            jax.ShapeDtypeStruct(mixer_proj.shape, BF16),
        ),
        16 << 20,
        1 << 28,
        place,
        far(expert_in),
        far(norm_gain.reshape(1, width)),
        far(route_ids.T),
        far(gate_in.T),
        far(conv_values.T),
        far(gate_out.T),
        far(mixer_proj),
        specs=[SMEM] + [HBM] * 7,
        scratch=[
            pltpu.VMEM((tokens, width), BF16),
            pltpu.VMEM((1, width), F32),
            pltpu.VMEM((choices, tokens), jnp.int32),
            pltpu.VMEM((channels, seq_len), BF16),
            pltpu.VMEM((channels, seq_len), BF16),
            pltpu.SemaphoreType.DMA((7,)),
        ],
    )
    halo = shifted(tail, "ep", 1)
    arrived = lax.all_to_all(sent, "ep", 0, 0, tiled=True)

    first = call(
        mixer_body,
        (jax.ShapeDtypeStruct((groups, seq_len, columns), BF16),) * turns,
        12 << 20,
        1 << 26,
        place_1,
        outer,
        product,
        conv_taps,
        halo,
        proj,
        specs=[SMEM] + [VMEM] * 5,
    )
    first = [first[0]] + [turned(first[d], TP[1], d) for d in range(1, turns)]

    own_block = arrived.reshape(1, slot_count, columns)
    copies = jnp.broadcast_to(own_block, (tp_count, slot_count, columns))
    gathered = lax.all_to_all(copies, TP, 0, 0, tiled=True)
    parts = call(
        lambda *refs: expert_body(slot_count // 4, *refs),
        pltpu.HBM((tp_count, slot_count, columns), BF16),
        24 << 20,
        1 << 32,
        gathered,
        gate_proj,
        up_proj,
        down_proj,
        scratch=[
            pltpu.VMEM((2, tp_count, slot_count // 4, columns), BF16),
            pltpu.SemaphoreType.DMA((2,)),
        ],
        place=HBM,
    )
    shared = lax.all_to_all(parts, TP, 0, 0, tiled=True)
    outputs = call(
        sum_body,
        jax.ShapeDtypeStruct((experts, capacity, columns), BF16),
        16 << 20,
        1 << 24,
        shared,
        scratch=[pltpu.VMEM((slot_count, columns), F32)],
    )
    returned = lax.all_to_all(outputs, "ep", 0, 0, tiled=True)

    second = call(
        regroup_body,
        (jax.ShapeDtypeStruct((seq_len, columns), BF16),) * groups,
        12 << 20,
        1 << 22,
        place_0,
        *first,
        specs=[SMEM] + [VMEM] * turns,
    )
    second = [second[0]] + [turned(second[d], TP[0], d) for d in range(1, groups)]
    mixed = call(
        final_body, jax.ShapeDtypeStruct((seq_len, columns), BF16), 8 << 20, 1 << 20, *second
    )
    expert_mix = call(
        combine_body,
        jax.ShapeDtypeStruct((tokens, columns), BF16),
        16 << 20,
        1 << 27,
        returned,
        slots.T,
        route_scores,
        scratch=[pltpu.VMEM((experts, stride, columns), F32)],
    )
    return (mixed, expert_mix)


def solution(mesh):
    torus = Mesh(mesh.devices.reshape(mesh.shape["ep"], 4, 4), ("ep", "tp_0", "tp_1"))
    in_specs = (
        P("ep", TP),
        P("ep", TP),
        P("ep", TP),
        P(None, TP),
        P(TP, None),
        P("ep", None),
        P(),
        P("ep", None),
        P("ep", None),
        P("ep", None, TP),
        P("ep", None, TP),
        P("ep", TP, None),
    )
    out_specs = (P("ep", TP), P("ep", TP))

    return jax.shard_map(
        shards, mesh=torus, in_specs=in_specs, out_specs=out_specs, check_vma=False
    )
```

```python
import jax
import jax.numpy as jnp
from jax import lax
from jax.experimental import pallas as pl
from jax.experimental.pallas import tpu as pltpu
from jax.sharding import Mesh
from jax.sharding import PartitionSpec as P


TP = ("tp_0", "tp_1")
F32 = jnp.float32
BF16 = jnp.bfloat16
VMEM = pl.BlockSpec(memory_space=pltpu.VMEM)
SMEM = pl.BlockSpec(memory_space=pltpu.SMEM)
HBM = pl.BlockSpec(memory_space=pltpu.HBM)


def shifted(block, axis, distance):
    devices = range(lax.axis_size(axis))
    route = [(i - distance, i) for i in devices if i - distance in devices]
    return lax.ppermute(block, axis, route)


def call(body, out, limit, flops, *operands, specs=None, scratch=(), place=None):
    return pl.pallas_call(
        body,
        out_shape=out,
        in_specs=specs or [VMEM] * len(operands),
        out_specs=jax.tree.map(lambda _: place or VMEM, out),
        scratch_shapes=scratch,
        compiler_params=pltpu.CompilerParams(vmem_limit_bytes=limit),
        cost_estimate=pl.CostEstimate(
            flops=flops, bytes_accessed=1 << 20, transcendentals=0
        ),
    )(*operands)


def far(array):
    return pltpu.with_memory_space_constraint(array, pltpu.HBM)


def dispatch_body(
    stride,
    experts,
    place,
    rows_far,
    gain_far,
    ids_far,
    inner_far,
    values_far,
    outer_far,
    proj_far,
    taps_far,
    sent,
    slots,
    tail,
    product,
    outer,
    proj,
    taps,
    rows,
    gain,
    ids,
    inner,
    values,
    done,
):
    pairs = (
        (rows_far, rows),
        (gain_far, gain),
        (ids_far, ids),
        (inner_far, inner),
        (values_far, values),
        (outer_far, outer),
        (proj_far, proj),
        (taps_far, taps),
    )
    copies = [
        pltpu.make_async_copy(there, here, done.at[n]) for n, (there, here) in enumerate(pairs)
    ]
    for copy in copies:
        copy.start()
    for copy in copies[3:5]:
        copy.wait()
    mixed = inner[...].astype(F32).T * values[...].astype(F32).T
    product[...] = mixed
    tail[...] = mixed[mixed.shape[0] - tail.shape[0] :, :]
    for copy in copies[:3] + copies[5:]:
        copy.wait()
    tokens, width = rows.shape
    capacity, columns = sent.shape[1:]
    wide = rows[...].astype(F32)
    scaling = lax.rsqrt(jnp.sum(wide * wide, axis=1, keepdims=True) / width + 1e-06)
    start = pl.multiple_of(place[0] * columns, columns)
    own = rows[:, pl.ds(start, columns)].astype(F32)
    normed = (own * scaling * gain[:, pl.ds(start, columns)]).astype(BF16)
    chosen = ids[...]
    expert = lax.broadcasted_iota(jnp.int32, (experts, tokens), 0)
    hits = [expert == chosen[k : k + 1, :] for k in range(chosen.shape[0])]
    marks = [jnp.where(h, 1.0, 0.0).astype(F32) for h in hits]
    total = marks[0]
    for m in marks[1:]:
        total = total + m
    earlier = lax.broadcasted_iota(jnp.int32, (tokens, tokens), 0)
    later = lax.broadcasted_iota(jnp.int32, (tokens, tokens), 1)
    before = jnp.dot(
        total.astype(BF16),
        jnp.where(earlier < later, 1.0, 0.0).astype(BF16),
        preferred_element_type=F32,
    )
    base = (expert * stride).astype(F32)
    where = [
        jnp.sum(m * (before + base), axis=0, keepdims=True).astype(jnp.int32) for m in marks
    ]
    slots[...] = jnp.concatenate(where, axis=0)
    slot = lax.broadcasted_iota(jnp.int32, (experts * stride, tokens), 0)
    table = slot == where[0]
    for w in where[1:]:
        table = table | (slot == w)
    placed = jnp.dot(
        jnp.where(table, 1.0, 0.0).astype(BF16), normed, preferred_element_type=F32
    ).reshape(experts, stride, columns)
    sent[...] = placed[:, :capacity, :].astype(BF16)


def expert_body(step, tokens, gate_w, up_w, down_w, out):
    blocks, rows, columns = tokens.shape

    def tile(number, carry):
        at = pl.ds(pl.multiple_of(number * step, step), step)
        left = jnp.concatenate([tokens[b, at, :] for b in range(blocks)], axis=1)
        gate = jnp.dot(left, gate_w[0], preferred_element_type=F32)
        up = jnp.dot(left, up_w[0], preferred_element_type=F32)
        hidden = (gate / (1.0 + jnp.exp(-gate)) * up).astype(BF16)
        part = jnp.dot(hidden, down_w[0], preferred_element_type=F32).astype(BF16)
        for b in range(blocks):
            out[b, at, :] = part[:, b * columns : (b + 1) * columns]
        return carry

    lax.fori_loop(0, rows // step, tile, 0)


def sum_body(parts, out, total):
    experts, capacity, _ = out.shape
    value = parts[0].astype(F32)
    for b in range(1, parts.shape[0]):
        value = value + parts[b].astype(F32)
    total[...] = value
    for e in range(experts):
        out[e] = total[e * capacity : (e + 1) * capacity, :].astype(BF16)


def mixer_body(place, outer, product_ref, taps, halo, proj, *outs):
    count = len(outs)
    groups, _, columns = outs[0].shape
    product = product_ref[...]
    row = lax.broadcasted_iota(jnp.int32, product.shape, 0)
    last = halo[1:2, :]
    back_one = jnp.where(row == 0, last, pltpu.roll(product, 1, 0))
    back_two = jnp.where(
        row == 0, halo[0:1, :], jnp.where(row == 1, last, pltpu.roll(product, 2, 0))
    )
    convolved = taps[0:1, :] * back_two + taps[1:2, :] * back_one + taps[2:3, :] * product
    branch = (outer[...].astype(F32).T * convolved).astype(BF16)
    for away, out in enumerate(outs):
        target = lax.rem(place[0] + away, count)
        for g in range(groups):
            start = pl.multiple_of((g * count + target) * columns, columns)
            out[g] = jnp.dot(
                branch, proj[:, pl.ds(start, columns)], preferred_element_type=F32
            ).astype(BF16)


def regroup_body(place, *refs):
    half = len(refs) // 2
    parts, outs = refs[:half], refs[half:]
    for away, out in enumerate(outs):
        target = lax.rem(place[0] + away, half)
        total = parts[0][target].astype(F32)
        for part in parts[1:]:
            total = total + part[target].astype(F32)
        out[...] = total.astype(BF16)


def final_body(*refs):
    total = refs[0][...].astype(F32)
    for part in refs[1:-1]:
        total = total + part[...].astype(F32)
    refs[-1][...] = total.astype(BF16)


def turned(block, axis, distance):
    count = lax.axis_size(axis)
    return lax.ppermute(block, axis, [(i, (i + distance) % count) for i in range(count)])


def combine_body(rows, slots, scores, out, padded):
    tokens = out.shape[0]
    experts, capacity, columns = rows.shape
    stride = padded.shape[1]
    slot = lax.broadcasted_iota(jnp.int32, (tokens, experts * stride), 1)
    padded[...] = jnp.zeros_like(padded)
    padded[:, :capacity, :] = rows[...].astype(F32)
    held = padded[...].reshape(experts * stride, columns).astype(BF16)
    score = scores[...]
    whole = jnp.sum(score, axis=1, keepdims=True)
    total = None
    for k in range(score.shape[1]):
        pick = jnp.where(slot == slots[:, k : k + 1], 1.0, 0.0).astype(BF16)
        term = jnp.dot(pick, held, preferred_element_type=F32)
        term = term * (score[:, k : k + 1] / whole)
        total = term if total is None else total + term
    out[...] = total.astype(BF16)


def shards(
    gate_out,
    gate_in,
    conv_values,
    conv_taps,
    mixer_proj,
    expert_in,
    norm_gain,
    route_ids,
    route_scores,
    gate_proj,
    up_proj,
    down_proj,
):
    tokens, choices = route_ids.shape
    width = expert_in.shape[1]
    ep_count = lax.axis_size("ep")
    tp_count = lax.axis_size(TP)
    local_experts = gate_proj.shape[0]
    experts = ep_count * local_experts
    capacity = max(2, (4 * tokens * choices + 3 * experts - 1) // (3 * experts))
    slot_count = experts * capacity
    stride = (capacity + 7) // 8 * 8
    columns = width // tp_count
    place = lax.axis_index(TP).astype(jnp.int32).reshape(1)
    place_0 = lax.axis_index(TP[0]).astype(jnp.int32).reshape(1)
    place_1 = lax.axis_index(TP[1]).astype(jnp.int32).reshape(1)
    groups = lax.axis_size(TP[0])
    turns = lax.axis_size(TP[1])
    seq_len = gate_in.shape[0]
    channels = gate_in.shape[1]

    sent, slots, tail, product, outer, proj, taps = call(
        lambda *refs: dispatch_body(stride, experts, *refs),
        (
            jax.ShapeDtypeStruct((experts, capacity, columns), BF16),
            jax.ShapeDtypeStruct((choices, tokens), jnp.int32),
            jax.ShapeDtypeStruct((conv_taps.shape[0] - 1, channels), F32),
            jax.ShapeDtypeStruct((seq_len, channels), F32),
            jax.ShapeDtypeStruct((channels, seq_len), BF16),
            jax.ShapeDtypeStruct(mixer_proj.shape, BF16),
            jax.ShapeDtypeStruct(conv_taps.shape, F32),
        ),
        16 << 20,
        1 << 28,
        place,
        far(expert_in),
        far(norm_gain.reshape(1, width)),
        far(route_ids.T),
        far(gate_in.T),
        far(conv_values.T),
        far(gate_out.T),
        far(mixer_proj),
        far(conv_taps),
        specs=[SMEM] + [HBM] * 8,
        scratch=[
            pltpu.VMEM((tokens, width), BF16),
            pltpu.VMEM((1, width), F32),
            pltpu.VMEM((choices, tokens), jnp.int32),
            pltpu.VMEM((channels, seq_len), BF16),
            pltpu.VMEM((channels, seq_len), BF16),
            pltpu.SemaphoreType.DMA((8,)),
        ],
    )
    halo = shifted(tail, "ep", 1)
    arrived = lax.all_to_all(sent, "ep", 0, 0, tiled=True)

    first = call(
        mixer_body,
        (jax.ShapeDtypeStruct((groups, seq_len, columns), BF16),) * turns,
        12 << 20,
        1 << 26,
        place_1,
        outer,
        product,
        taps,
        halo,
        proj,
        specs=[SMEM] + [VMEM] * 5,
    )
    first = [first[0]] + [turned(first[d], TP[1], d) for d in range(1, turns)]

    own_block = arrived.reshape(1, slot_count, columns)
    copies = jnp.broadcast_to(own_block, (tp_count, slot_count, columns))
    gathered = lax.all_to_all(copies, TP, 0, 0, tiled=True)
    parts = call(
        lambda *refs: expert_body(slot_count // 4, *refs),
        jax.ShapeDtypeStruct((tp_count, slot_count, columns), BF16),
        24 << 20,
        1 << 32,
        gathered,
        gate_proj,
        up_proj,
        down_proj,
    )
    shared = lax.all_to_all(parts, TP, 0, 0, tiled=True)
    outputs = call(
        sum_body,
        jax.ShapeDtypeStruct((experts, capacity, columns), BF16),
        16 << 20,
        1 << 24,
        shared,
        scratch=[pltpu.VMEM((slot_count, columns), F32)],
    )
    returned = lax.all_to_all(outputs, "ep", 0, 0, tiled=True)

    second = call(
        regroup_body,
        (jax.ShapeDtypeStruct((seq_len, columns), BF16),) * groups,
        12 << 20,
        1 << 22,
        place_0,
        *first,
        specs=[SMEM] + [VMEM] * turns,
    )
    second = [second[0]] + [turned(second[d], TP[0], d) for d in range(1, groups)]
    mixed = call(
        final_body, jax.ShapeDtypeStruct((seq_len, columns), BF16), 8 << 20, 1 << 20, *second
    )
    expert_mix = call(
        combine_body,
        jax.ShapeDtypeStruct((tokens, columns), BF16),
        16 << 20,
        1 << 27,
        returned,
        slots.T,
        route_scores,
        scratch=[pltpu.VMEM((experts, stride, columns), F32)],
    )
    return (mixed, expert_mix)


def solution(mesh):
    torus = Mesh(mesh.devices.reshape(mesh.shape["ep"], 4, 4), ("ep", "tp_0", "tp_1"))
    in_specs = (
        P("ep", TP),
        P("ep", TP),
        P("ep", TP),
        P(None, TP),
        P(TP, None),
        P("ep", None),
        P(),
        P("ep", None),
        P("ep", None),
        P("ep", None, TP),
        P("ep", None, TP),
        P("ep", TP, None),
    )
    out_specs = (P("ep", TP), P("ep", TP))

    return jax.shard_map(
        shards, mesh=torus, in_specs=in_specs, out_specs=out_specs, check_vma=False
    )
```

```python
import jax
import jax.numpy as jnp
from jax import lax
from jax.experimental import pallas as pl
from jax.experimental.pallas import tpu as pltpu
from jax.sharding import Mesh
from jax.sharding import PartitionSpec as P


TP = ("tp_0", "tp_1")
F32 = jnp.float32
BF16 = jnp.bfloat16
VMEM = pl.BlockSpec(memory_space=pltpu.VMEM)
SMEM = pl.BlockSpec(memory_space=pltpu.SMEM)
HBM = pl.BlockSpec(memory_space=pltpu.HBM)


def shifted(block, axis, distance):
    devices = range(lax.axis_size(axis))
    route = [(i - distance, i) for i in devices if i - distance in devices]
    return lax.ppermute(block, axis, route)


def call(body, out, limit, flops, *operands, specs=None, scratch=(), place=None):
    return pl.pallas_call(
        body,
        out_shape=out,
        in_specs=specs or [VMEM] * len(operands),
        out_specs=jax.tree.map(lambda _: place or VMEM, out),
        scratch_shapes=scratch,
        compiler_params=pltpu.CompilerParams(vmem_limit_bytes=limit),
        cost_estimate=pl.CostEstimate(
            flops=flops, bytes_accessed=1 << 20, transcendentals=0
        ),
    )(*operands)


def far(array):
    return pltpu.with_memory_space_constraint(array, pltpu.HBM)


def dispatch_body(
    stride,
    experts,
    place,
    rows_far,
    gain_far,
    ids_far,
    inner_far,
    values_far,
    outer_far,
    proj_far,
    taps_far,
    sent,
    slots,
    tail,
    product,
    outer,
    proj,
    taps,
    rows,
    gain,
    ids,
    inner,
    values,
    done,
):
    pairs = (
        (rows_far, rows),
        (gain_far, gain),
        (ids_far, ids),
        (inner_far, inner),
        (values_far, values),
        (outer_far, outer),
        (proj_far, proj),
        (taps_far, taps),
    )
    copies = [
        pltpu.make_async_copy(there, here, done.at[n]) for n, (there, here) in enumerate(pairs)
    ]
    for copy in copies:
        copy.start()
    for copy in copies[3:5]:
        copy.wait()
    mixed = inner[...].astype(F32).T * values[...].astype(F32).T
    product[...] = mixed
    tail[...] = mixed[mixed.shape[0] - tail.shape[0] :, :]
    for copy in copies[:3] + copies[5:]:
        copy.wait()
    tokens, width = rows.shape
    capacity, columns = sent.shape[1:]
    wide = rows[...].astype(F32)
    scaling = lax.rsqrt(jnp.sum(wide * wide, axis=1, keepdims=True) / width + 1e-06)
    start = pl.multiple_of(place[0] * columns, columns)
    own = rows[:, pl.ds(start, columns)].astype(F32)
    normed = (own * scaling * gain[:, pl.ds(start, columns)]).astype(BF16)
    chosen = ids[...]
    expert = lax.broadcasted_iota(jnp.int32, (experts, tokens), 0)
    hits = [expert == chosen[k : k + 1, :] for k in range(chosen.shape[0])]
    marks = [jnp.where(h, 1.0, 0.0).astype(F32) for h in hits]
    total = marks[0]
    for m in marks[1:]:
        total = total + m
    earlier = lax.broadcasted_iota(jnp.int32, (tokens, tokens), 0)
    later = lax.broadcasted_iota(jnp.int32, (tokens, tokens), 1)
    before = jnp.dot(
        total.astype(BF16),
        jnp.where(earlier < later, 1.0, 0.0).astype(BF16),
        preferred_element_type=F32,
    )
    base = (expert * stride).astype(F32)
    where = [
        jnp.sum(m * (before + base), axis=0, keepdims=True).astype(jnp.int32) for m in marks
    ]
    slots[...] = jnp.concatenate(where, axis=0)
    slot = lax.broadcasted_iota(jnp.int32, (experts * stride, tokens), 0)
    table = slot == where[0]
    for w in where[1:]:
        table = table | (slot == w)
    placed = jnp.dot(
        jnp.where(table, 1.0, 0.0).astype(BF16), normed, preferred_element_type=F32
    ).reshape(experts, stride, columns)
    sent[...] = placed[:, :capacity, :].astype(BF16)


def expert_body(step, core, tokens, gate_w, up_w, down_w, out):
    sides, blocks, rows, columns = tokens.shape[0], tokens.shape[1], *tokens.shape[2:]
    even = core[0] == 0

    def tile(number, carry):
        at = pl.ds(pl.multiple_of(number * step, step), step)
        left = []
        for y in range(sides):
            for x in range(blocks):
                first, second = jnp.where(even, y, x), jnp.where(even, x, y)
                left.append(tokens[first, second, at, :])
        left = jnp.concatenate(left, axis=1)
        gate = jnp.dot(left, gate_w[0], preferred_element_type=F32)
        up = jnp.dot(left, up_w[0], preferred_element_type=F32)
        hidden = (gate / (1.0 + jnp.exp(-gate)) * up).astype(BF16)
        part = jnp.dot(hidden, down_w[0], preferred_element_type=F32).astype(BF16)
        for y in range(sides):
            for x in range(blocks):
                first, second = jnp.where(even, x, y), jnp.where(even, y, x)
                start = (y * blocks + x) * columns
                out[first, second, at, :] = part[:, start : start + columns]
        return carry

    lax.fori_loop(0, rows // step, tile, 0)


def fold_body(parts, out):
    value = parts[0].astype(F32)
    for b in range(1, parts.shape[0]):
        value = value + parts[b].astype(F32)
    out[...] = value.astype(BF16)


def sum_body(parts, out, total):
    experts, capacity, _ = out.shape
    value = parts[0].astype(F32)
    for b in range(1, parts.shape[0]):
        value = value + parts[b].astype(F32)
    total[...] = value
    for e in range(experts):
        out[e] = total[e * capacity : (e + 1) * capacity, :].astype(BF16)


def mixer_body(place, outer, product_ref, taps, halo, proj, *outs):
    count = len(outs)
    groups, _, columns = outs[0].shape
    product = product_ref[...]
    row = lax.broadcasted_iota(jnp.int32, product.shape, 0)
    last = halo[1:2, :]
    back_one = jnp.where(row == 0, last, pltpu.roll(product, 1, 0))
    back_two = jnp.where(
        row == 0, halo[0:1, :], jnp.where(row == 1, last, pltpu.roll(product, 2, 0))
    )
    convolved = taps[0:1, :] * back_two + taps[1:2, :] * back_one + taps[2:3, :] * product
    branch = (outer[...].astype(F32).T * convolved).astype(BF16)
    for away, out in enumerate(outs):
        target = lax.rem(place[0] + away, count)
        for g in range(groups):
            start = pl.multiple_of((g * count + target) * columns, columns)
            out[g] = jnp.dot(
                branch, proj[:, pl.ds(start, columns)], preferred_element_type=F32
            ).astype(BF16)


def regroup_body(place, *refs):
    half = len(refs) // 2
    parts, outs = refs[:half], refs[half:]
    for away, out in enumerate(outs):
        target = lax.rem(place[0] + away, half)
        total = parts[0][target].astype(F32)
        for part in parts[1:]:
            total = total + part[target].astype(F32)
        out[...] = total.astype(BF16)


def final_body(*refs):
    total = refs[0][...].astype(F32)
    for part in refs[1:-1]:
        total = total + part[...].astype(F32)
    refs[-1][...] = total.astype(BF16)


def crossed(block, stage):
    names = ("ep",) + TP
    eps, ys, xs = (lax.axis_size(name) for name in names)
    groups = []
    for e in range(eps):
        if (e + stage) % 2 == 0:
            groups += [[(e * ys + y) * xs + x for x in range(xs)] for y in range(ys)]
        else:
            groups += [[(e * ys + y) * xs + x for y in range(ys)] for x in range(xs)]
    return lax.all_to_all(block, names, 0, 0, axis_index_groups=groups, tiled=True)


def turned(block, axis, distance):
    count = lax.axis_size(axis)
    return lax.ppermute(block, axis, [(i, (i + distance) % count) for i in range(count)])


def combine_body(rows, slots, scores, out, padded):
    tokens = out.shape[0]
    experts, capacity, columns = rows.shape
    stride = padded.shape[1]
    slot = lax.broadcasted_iota(jnp.int32, (tokens, experts * stride), 1)
    padded[...] = jnp.zeros_like(padded)
    padded[:, :capacity, :] = rows[...].astype(F32)
    held = padded[...].reshape(experts * stride, columns).astype(BF16)
    score = scores[...]
    whole = jnp.sum(score, axis=1, keepdims=True)
    total = None
    for k in range(score.shape[1]):
        pick = jnp.where(slot == slots[:, k : k + 1], 1.0, 0.0).astype(BF16)
        term = jnp.dot(pick, held, preferred_element_type=F32)
        term = term * (score[:, k : k + 1] / whole)
        total = term if total is None else total + term
    out[...] = total.astype(BF16)


def shards(
    gate_out,
    gate_in,
    conv_values,
    conv_taps,
    mixer_proj,
    expert_in,
    norm_gain,
    route_ids,
    route_scores,
    gate_proj,
    up_proj,
    down_proj,
):
    tokens, choices = route_ids.shape
    width = expert_in.shape[1]
    ep_count = lax.axis_size("ep")
    tp_count = lax.axis_size(TP)
    local_experts = gate_proj.shape[0]
    experts = ep_count * local_experts
    capacity = max(2, (4 * tokens * choices + 3 * experts - 1) // (3 * experts))
    slot_count = experts * capacity
    stride = (capacity + 7) // 8 * 8
    columns = width // tp_count
    place = lax.axis_index(TP).astype(jnp.int32).reshape(1)
    place_0 = lax.axis_index(TP[0]).astype(jnp.int32).reshape(1)
    place_1 = lax.axis_index(TP[1]).astype(jnp.int32).reshape(1)
    groups = lax.axis_size(TP[0])
    turns = lax.axis_size(TP[1])
    seq_len = gate_in.shape[0]
    channels = gate_in.shape[1]

    sent, slots, tail, product, outer, proj, taps = call(
        lambda *refs: dispatch_body(stride, experts, *refs),
        (
            jax.ShapeDtypeStruct((experts, capacity, columns), BF16),
            jax.ShapeDtypeStruct((choices, tokens), jnp.int32),
            jax.ShapeDtypeStruct((conv_taps.shape[0] - 1, channels), F32),
            jax.ShapeDtypeStruct((seq_len, channels), F32),
            jax.ShapeDtypeStruct((channels, seq_len), BF16),
            jax.ShapeDtypeStruct(mixer_proj.shape, BF16),
            jax.ShapeDtypeStruct(conv_taps.shape, F32),
        ),
        16 << 20,
        1 << 28,
        place,
        far(expert_in),
        far(norm_gain.reshape(1, width)),
        far(route_ids.T),
        far(gate_in.T),
        far(conv_values.T),
        far(gate_out.T),
        far(mixer_proj),
        far(conv_taps),
        specs=[SMEM] + [HBM] * 8,
        scratch=[
            pltpu.VMEM((tokens, width), BF16),
            pltpu.VMEM((1, width), F32),
            pltpu.VMEM((choices, tokens), jnp.int32),
            pltpu.VMEM((channels, seq_len), BF16),
            pltpu.VMEM((channels, seq_len), BF16),
            pltpu.SemaphoreType.DMA((8,)),
        ],
    )
    halo = shifted(tail, "ep", 1)
    arrived = lax.all_to_all(sent, "ep", 0, 0, tiled=True)

    first = call(
        mixer_body,
        (jax.ShapeDtypeStruct((groups, seq_len, columns), BF16),) * turns,
        12 << 20,
        1 << 26,
        place_1,
        outer,
        product,
        taps,
        halo,
        proj,
        specs=[SMEM] + [VMEM] * 5,
    )
    first = [first[0]] + [turned(first[d], TP[1], d) for d in range(1, turns)]

    side = lax.axis_size(TP[0])
    block = (slot_count, columns)
    core = (lax.axis_index("ep") % 2).astype(jnp.int32).reshape(1)
    own_block = jnp.broadcast_to(arrived.reshape(1, *block), (side, *block))
    own_block, core = lax.optimization_barrier((own_block, core))
    line = crossed(own_block, 0)
    line = jnp.broadcast_to(line[None], (side, side, *block))
    gathered = crossed(line, 1)
    parts = call(
        lambda *refs: expert_body(slot_count // 4, *refs),
        jax.ShapeDtypeStruct((side, side, *block), BF16),
        24 << 20,
        1 << 32,
        core,
        gathered,
        gate_proj,
        up_proj,
        down_proj,
        specs=[SMEM] + [VMEM] * 4,
    )
    line = crossed(parts, 0)
    line = call(fold_body, jax.ShapeDtypeStruct((side, *block), BF16), 16 << 20, 1 << 24, line)
    shared = crossed(line, 1)
    outputs = call(
        sum_body,
        jax.ShapeDtypeStruct((experts, capacity, columns), BF16),
        16 << 20,
        1 << 24,
        shared,
        scratch=[pltpu.VMEM((slot_count, columns), F32)],
    )
    returned = lax.all_to_all(outputs, "ep", 0, 0, tiled=True)

    second = call(
        regroup_body,
        (jax.ShapeDtypeStruct((seq_len, columns), BF16),) * groups,
        12 << 20,
        1 << 22,
        place_0,
        *first,
        specs=[SMEM] + [VMEM] * turns,
    )
    second = [second[0]] + [turned(second[d], TP[0], d) for d in range(1, groups)]
    mixed = call(
        final_body, jax.ShapeDtypeStruct((seq_len, columns), BF16), 8 << 20, 1 << 20, *second
    )
    expert_mix = call(
        combine_body,
        jax.ShapeDtypeStruct((tokens, columns), BF16),
        16 << 20,
        1 << 27,
        returned,
        slots.T,
        route_scores,
        scratch=[pltpu.VMEM((experts, stride, columns), F32)],
    )
    return (mixed, expert_mix)


def solution(mesh):
    torus = Mesh(mesh.devices.reshape(mesh.shape["ep"], 4, 4), ("ep", "tp_0", "tp_1"))
    in_specs = (
        P("ep", TP),
        P("ep", TP),
        P("ep", TP),
        P(None, TP),
        P(TP, None),
        P("ep", None),
        P(),
        P("ep", None),
        P("ep", None),
        P("ep", None, TP),
        P("ep", None, TP),
        P("ep", TP, None),
    )
    out_specs = (P("ep", TP), P("ep", TP))

    return jax.shard_map(
        shards, mesh=torus, in_specs=in_specs, out_specs=out_specs, check_vma=False
    )
```

```python
import jax
import jax.numpy as jnp
from jax import lax
from jax.experimental import pallas as pl
from jax.experimental.pallas import tpu as pltpu
from jax.sharding import Mesh
from jax.sharding import PartitionSpec as P


TP = ("tp_0", "tp_1")
F32 = jnp.float32
BF16 = jnp.bfloat16
VMEM = pl.BlockSpec(memory_space=pltpu.VMEM)
SMEM = pl.BlockSpec(memory_space=pltpu.SMEM)
HBM = pl.BlockSpec(memory_space=pltpu.HBM)


def shifted(block, axis, distance):
    devices = range(lax.axis_size(axis))
    route = [(i - distance, i) for i in devices if i - distance in devices]
    return lax.ppermute(block, axis, route)


def call(body, out, limit, flops, *operands, specs=None, scratch=(), place=None):
    return pl.pallas_call(
        body,
        out_shape=out,
        in_specs=specs or [VMEM] * len(operands),
        out_specs=jax.tree.map(lambda _: place or VMEM, out),
        scratch_shapes=scratch,
        compiler_params=pltpu.CompilerParams(vmem_limit_bytes=limit),
        cost_estimate=pl.CostEstimate(
            flops=flops, bytes_accessed=1 << 20, transcendentals=0
        ),
    )(*operands)


def far(array):
    return pltpu.with_memory_space_constraint(array, pltpu.HBM)


def dispatch_body(
    stride,
    experts,
    place,
    rows_far,
    gain_far,
    ids_far,
    inner_far,
    values_far,
    outer_far,
    proj_far,
    taps_far,
    sent,
    slots,
    tail,
    product,
    outer,
    proj,
    taps,
    rows,
    gain,
    ids,
    inner,
    values,
    done,
):
    pairs = (
        (rows_far, rows),
        (gain_far, gain),
        (ids_far, ids),
        (inner_far, inner),
        (values_far, values),
        (outer_far, outer),
        (proj_far, proj),
        (taps_far, taps),
    )
    copies = [
        pltpu.make_async_copy(there, here, done.at[n]) for n, (there, here) in enumerate(pairs)
    ]
    for copy in copies:
        copy.start()
    for copy in copies[3:5]:
        copy.wait()
    mixed = inner[...].astype(F32).T * values[...].astype(F32).T
    product[...] = mixed
    tail[...] = mixed[mixed.shape[0] - tail.shape[0] :, :]
    for copy in copies[:3] + copies[5:]:
        copy.wait()
    tokens, width = rows.shape
    capacity, columns = sent.shape[1:]
    wide = rows[...].astype(F32)
    scaling = lax.rsqrt(jnp.sum(wide * wide, axis=1, keepdims=True) / width + 1e-06)
    start = pl.multiple_of(place[0] * columns, columns)
    own = rows[:, pl.ds(start, columns)].astype(F32)
    normed = (own * scaling * gain[:, pl.ds(start, columns)]).astype(BF16)
    chosen = ids[...]
    expert = lax.broadcasted_iota(jnp.int32, (experts, tokens), 0)
    hits = [expert == chosen[k : k + 1, :] for k in range(chosen.shape[0])]
    marks = [jnp.where(h, 1.0, 0.0).astype(F32) for h in hits]
    total = marks[0]
    for m in marks[1:]:
        total = total + m
    earlier = lax.broadcasted_iota(jnp.int32, (tokens, tokens), 0)
    later = lax.broadcasted_iota(jnp.int32, (tokens, tokens), 1)
    before = jnp.dot(
        total.astype(BF16),
        jnp.where(earlier < later, 1.0, 0.0).astype(BF16),
        preferred_element_type=F32,
    )
    base = (expert * stride).astype(F32)
    where = [
        jnp.sum(m * (before + base), axis=0, keepdims=True).astype(jnp.int32) for m in marks
    ]
    slots[...] = jnp.concatenate(where, axis=0)
    slot = lax.broadcasted_iota(jnp.int32, (experts * stride, tokens), 0)
    table = slot == where[0]
    for w in where[1:]:
        table = table | (slot == w)
    placed = jnp.dot(
        jnp.where(table, 1.0, 0.0).astype(BF16), normed, preferred_element_type=F32
    ).reshape(experts, stride, columns)
    sent[...] = placed[:, :capacity, :].astype(BF16)


def weights_body(order, gate_far, up_far, down_far, gate_w, up_w, down_w, done):
    count = order.shape[0]
    columns = gate_w.shape[0] // count
    copies = []
    for p in range(count):
        near = pl.ds(p * columns, columns)
        there = pl.ds(pl.multiple_of(order[p] * columns, columns), columns)
        for n, (source, target) in enumerate(
            (
                (gate_far.at[0, there, :], gate_w.at[near, :]),
                (up_far.at[0, there, :], up_w.at[near, :]),
                (down_far.at[0, :, there], down_w.at[:, near]),
            )
        ):
            copies.append(pltpu.make_async_copy(source, target, done.at[3 * p + n]))
            copies[-1].start()
    for copy in copies:
        copy.wait()


def expert_body(step, *refs):
    sides = (len(refs) - 3) // 2
    tokens, outs = refs[:sides], refs[sides + 3 :]
    gate_w, up_w, down_w = refs[sides : sides + 3]
    blocks, rows, columns = tokens[0].shape
    spots = [(n, m) for n in range(sides) for m in range(blocks)]

    def tile(number, carry):
        at = pl.ds(pl.multiple_of(number * step, step), step)
        left = jnp.concatenate([tokens[n][m, at, :] for n, m in spots], axis=1)
        gate = jnp.dot(left, gate_w[...], preferred_element_type=F32)
        up = jnp.dot(left, up_w[...], preferred_element_type=F32)
        hidden = (gate / (1.0 + jnp.exp(-gate)) * up).astype(BF16)
        part = jnp.dot(hidden, down_w[...], preferred_element_type=F32).astype(BF16)
        for p, (n, m) in enumerate(spots):
            outs[n][m, at, :] = part[:, p * columns : (p + 1) * columns]
        return carry

    lax.fori_loop(0, rows // step, tile, 0)


def fold_body(*refs):
    value = refs[0][...].astype(F32)
    for part in refs[1:-1]:
        value = value + part[...].astype(F32)
    refs[-1][...] = value.astype(BF16)


def sum_body(parts, out, total):
    experts, capacity, _ = out.shape
    value = parts[0].astype(F32)
    for b in range(1, parts.shape[0]):
        value = value + parts[b].astype(F32)
    total[...] = value
    for e in range(experts):
        out[e] = total[e * capacity : (e + 1) * capacity, :].astype(BF16)


def mixer_body(place, outer, product_ref, taps, halo, proj, *outs):
    count = len(outs)
    groups, _, columns = outs[0].shape
    product = product_ref[...]
    row = lax.broadcasted_iota(jnp.int32, product.shape, 0)
    last = halo[1:2, :]
    back_one = jnp.where(row == 0, last, pltpu.roll(product, 1, 0))
    back_two = jnp.where(
        row == 0, halo[0:1, :], jnp.where(row == 1, last, pltpu.roll(product, 2, 0))
    )
    convolved = taps[0:1, :] * back_two + taps[1:2, :] * back_one + taps[2:3, :] * product
    branch = (outer[...].astype(F32).T * convolved).astype(BF16)
    for away, out in enumerate(outs):
        target = lax.rem(place[0] + away, count)
        for g in range(groups):
            start = pl.multiple_of((g * count + target) * columns, columns)
            out[g] = jnp.dot(
                branch, proj[:, pl.ds(start, columns)], preferred_element_type=F32
            ).astype(BF16)


def regroup_body(place, *refs):
    half = len(refs) // 2
    parts, outs = refs[:half], refs[half:]
    for away, out in enumerate(outs):
        target = lax.rem(place[0] + away, half)
        total = parts[0][target].astype(F32)
        for part in parts[1:]:
            total = total + part[target].astype(F32)
        out[...] = total.astype(BF16)


def final_body(*refs):
    total = refs[0][...].astype(F32)
    for part in refs[1:-1]:
        total = total + part[...].astype(F32)
    refs[-1][...] = total.astype(BF16)


PAIRS = (((1, 2), (3, 0)), ((0, 1), (2, 3)))


def squares(pairing):
    return [[(y, x) for y in ys for x in xs] for ys in PAIRS[pairing] for xs in PAIRS[pairing]]


def crossed(block, stage):
    names = ("ep",) + TP
    eps, _, xs = (lax.axis_size(name) for name in names)
    groups = []
    for e in range(eps):
        for square in squares((e + stage) % 2):
            groups.append([(e * xs + y) * xs + x for y, x in square])
    return lax.all_to_all(block, names, 0, 0, axis_index_groups=groups, tiled=True)


def flipped(spot, stage, flip):
    pair = {}
    for low, high in PAIRS[stage]:
        pair[low], pair[high] = high, low
    return (pair[spot[0]] if flip & 2 else spot[0], pair[spot[1]] if flip & 1 else spot[1])


def arrivals(side):
    rows = []
    for core in range(2):
        for y in range(side):
            for x in range(side):
                row = []
                for flip in range(4):
                    member = flipped((y, x), (core + 1) % 2, flip)
                    group = next(g for g in squares(core % 2) if member in g)
                    row += [there_y * side + there_x for there_y, there_x in group]
                rows.append(row)
    return rows


def swapped(block, flip):
    names = ("ep",) + TP
    eps, ys, xs = (lax.axis_size(name) for name in names)
    route = []
    for e in range(eps):
        for y in range(ys):
            for x in range(xs):
                to_y, to_x = flipped((y, x), (e + 1) % 2, flip)
                route.append(((e * ys + y) * xs + x, (e * ys + to_y) * xs + to_x))
    return lax.ppermute(block, names, route)


def turned(block, axis, distance):
    count = lax.axis_size(axis)
    return lax.ppermute(block, axis, [(i, (i + distance) % count) for i in range(count)])


def combine_body(rows, slots, scores, out, padded):
    tokens = out.shape[0]
    experts, capacity, columns = rows.shape
    stride = padded.shape[1]
    slot = lax.broadcasted_iota(jnp.int32, (tokens, experts * stride), 1)
    padded[...] = jnp.zeros_like(padded)
    padded[:, :capacity, :] = rows[...].astype(F32)
    held = padded[...].reshape(experts * stride, columns).astype(BF16)
    score = scores[...]
    whole = jnp.sum(score, axis=1, keepdims=True)
    total = None
    for k in range(score.shape[1]):
        pick = jnp.where(slot == slots[:, k : k + 1], 1.0, 0.0).astype(BF16)
        term = jnp.dot(pick, held, preferred_element_type=F32)
        term = term * (score[:, k : k + 1] / whole)
        total = term if total is None else total + term
    out[...] = total.astype(BF16)


def shards(
    gate_out,
    gate_in,
    conv_values,
    conv_taps,
    mixer_proj,
    expert_in,
    norm_gain,
    route_ids,
    route_scores,
    gate_proj,
    up_proj,
    down_proj,
):
    tokens, choices = route_ids.shape
    width = expert_in.shape[1]
    ep_count = lax.axis_size("ep")
    tp_count = lax.axis_size(TP)
    local_experts = gate_proj.shape[0]
    experts = ep_count * local_experts
    capacity = max(2, (4 * tokens * choices + 3 * experts - 1) // (3 * experts))
    slot_count = experts * capacity
    stride = (capacity + 7) // 8 * 8
    columns = width // tp_count
    place = lax.axis_index(TP).astype(jnp.int32).reshape(1)
    place_0 = lax.axis_index(TP[0]).astype(jnp.int32).reshape(1)
    place_1 = lax.axis_index(TP[1]).astype(jnp.int32).reshape(1)
    groups = lax.axis_size(TP[0])
    turns = lax.axis_size(TP[1])
    seq_len = gate_in.shape[0]
    channels = gate_in.shape[1]

    sent, slots, tail, product, outer, proj, taps = call(
        lambda *refs: dispatch_body(stride, experts, *refs),
        (
            jax.ShapeDtypeStruct((experts, capacity, columns), BF16),
            jax.ShapeDtypeStruct((choices, tokens), jnp.int32),
            jax.ShapeDtypeStruct((conv_taps.shape[0] - 1, channels), F32),
            jax.ShapeDtypeStruct((seq_len, channels), F32),
            jax.ShapeDtypeStruct((channels, seq_len), BF16),
            jax.ShapeDtypeStruct(mixer_proj.shape, BF16),
            jax.ShapeDtypeStruct(conv_taps.shape, F32),
        ),
        16 << 20,
        1 << 28,
        place,
        far(expert_in),
        far(norm_gain.reshape(1, width)),
        far(route_ids.T),
        far(gate_in.T),
        far(conv_values.T),
        far(gate_out.T),
        far(mixer_proj),
        far(conv_taps),
        specs=[SMEM] + [HBM] * 8,
        scratch=[
            pltpu.VMEM((tokens, width), BF16),
            pltpu.VMEM((1, width), F32),
            pltpu.VMEM((choices, tokens), jnp.int32),
            pltpu.VMEM((channels, seq_len), BF16),
            pltpu.VMEM((channels, seq_len), BF16),
            pltpu.SemaphoreType.DMA((8,)),
        ],
    )
    halo = shifted(tail, "ep", 1)
    arrived = lax.all_to_all(sent, "ep", 0, 0, tiled=True)

    first = call(
        mixer_body,
        (jax.ShapeDtypeStruct((groups, seq_len, columns), BF16),) * turns,
        12 << 20,
        1 << 26,
        place_1,
        outer,
        product,
        taps,
        halo,
        proj,
        specs=[SMEM] + [VMEM] * 5,
    )
    first = [first[0]] + [turned(first[d], TP[1], d) for d in range(1, turns)]

    side = lax.axis_size(TP[0])
    block = (slot_count, columns)
    table = jnp.array(arrivals(side), jnp.int32)
    core = lax.axis_index("ep") % 2
    order = lax.dynamic_index_in_dim(
        table, core * tp_count + lax.axis_index(TP), keepdims=False
    )
    own_block = jnp.broadcast_to(arrived.reshape(1, *block), (side, *block))
    own_block, order = lax.optimization_barrier((own_block, order))
    line = crossed(own_block, 0)
    lines = [line]
    for flip in (1, 2, 3):
        lines.append(swapped(line, flip))
    weights = call(
        weights_body,
        tuple(
            jax.ShapeDtypeStruct(w.shape[1:], BF16) for w in (gate_proj, up_proj, down_proj)
        ),
        8 << 20,
        1 << 22,
        order,
        far(gate_proj),
        far(up_proj),
        far(down_proj),
        specs=[SMEM, HBM, HBM, HBM],
        scratch=[pltpu.SemaphoreType.DMA((3 * tp_count,))],
    )
    parts = call(
        lambda *refs: expert_body(slot_count // 2, *refs),
        (jax.ShapeDtypeStruct((side, *block), BF16),) * side,
        24 << 20,
        1 << 32,
        *lines,
        *weights,
    )
    parts = list(parts)
    for flip in (1, 2, 3):
        parts[flip] = swapped(parts[flip], flip)
    line = call(
        fold_body,
        jax.ShapeDtypeStruct((side, *block), BF16),
        16 << 20,
        1 << 24,
        *parts,
    )
    shared = crossed(line, 0)
    outputs = call(
        sum_body,
        jax.ShapeDtypeStruct((experts, capacity, columns), BF16),
        16 << 20,
        1 << 24,
        shared,
        scratch=[pltpu.VMEM((slot_count, columns), F32)],
    )
    returned = lax.all_to_all(outputs, "ep", 0, 0, tiled=True)

    second = call(
        regroup_body,
        (jax.ShapeDtypeStruct((seq_len, columns), BF16),) * groups,
        12 << 20,
        1 << 22,
        place_0,
        *first,
        specs=[SMEM] + [VMEM] * turns,
    )
    second = [second[0]] + [turned(second[d], TP[0], d) for d in range(1, groups)]
    mixed = call(
        final_body, jax.ShapeDtypeStruct((seq_len, columns), BF16), 8 << 20, 1 << 20, *second
    )
    expert_mix = call(
        combine_body,
        jax.ShapeDtypeStruct((tokens, columns), BF16),
        16 << 20,
        1 << 27,
        returned,
        slots.T,
        route_scores,
        scratch=[pltpu.VMEM((experts, stride, columns), F32)],
    )
    return (mixed, expert_mix)


def solution(mesh):
    torus = Mesh(mesh.devices.reshape(mesh.shape["ep"], 4, 4), ("ep", "tp_0", "tp_1"))
    in_specs = (
        P("ep", TP),
        P("ep", TP),
        P("ep", TP),
        P(None, TP),
        P(TP, None),
        P("ep", None),
        P(),
        P("ep", None),
        P("ep", None),
        P("ep", None, TP),
        P("ep", None, TP),
        P("ep", TP, None),
    )
    out_specs = (P("ep", TP), P("ep", TP))

    return jax.shard_map(
        shards, mesh=torus, in_specs=in_specs, out_specs=out_specs, check_vma=False
    )
```

```python
import jax
import jax.numpy as jnp
from jax import lax
from jax.experimental import pallas as pl
from jax.experimental.pallas import tpu as pltpu
from jax.sharding import Mesh
from jax.sharding import PartitionSpec as P


TP = ("tp_0", "tp_1")
F32 = jnp.float32
BF16 = jnp.bfloat16
VMEM = pl.BlockSpec(memory_space=pltpu.VMEM)
SMEM = pl.BlockSpec(memory_space=pltpu.SMEM)
HBM = pl.BlockSpec(memory_space=pltpu.HBM)


def shifted(block, axis, distance):
    devices = range(lax.axis_size(axis))
    route = [(i - distance, i) for i in devices if i - distance in devices]
    return lax.ppermute(block, axis, route)


def call(body, out, limit, flops, *operands, specs=None, scratch=(), place=None):
    return pl.pallas_call(
        body,
        out_shape=out,
        in_specs=specs or [VMEM] * len(operands),
        out_specs=jax.tree.map(lambda _: place or VMEM, out),
        scratch_shapes=scratch,
        compiler_params=pltpu.CompilerParams(vmem_limit_bytes=limit),
        cost_estimate=pl.CostEstimate(
            flops=flops, bytes_accessed=1 << 20, transcendentals=0
        ),
    )(*operands)


def far(array):
    return pltpu.with_memory_space_constraint(array, pltpu.HBM)


def dispatch_body(
    stride,
    experts,
    place,
    rows_far,
    gain_far,
    ids_far,
    inner_far,
    values_far,
    outer_far,
    proj_far,
    taps_far,
    sent,
    slots,
    tail,
    product,
    outer,
    proj,
    taps,
    rows,
    gain,
    ids,
    inner,
    values,
    done,
):
    pairs = (
        (rows_far, rows),
        (gain_far, gain),
        (ids_far, ids),
        (inner_far, inner),
        (values_far, values),
        (outer_far, outer),
        (proj_far, proj),
        (taps_far, taps),
    )
    copies = [
        pltpu.make_async_copy(there, here, done.at[n]) for n, (there, here) in enumerate(pairs)
    ]
    for copy in copies:
        copy.start()
    for copy in copies[3:5]:
        copy.wait()
    mixed = inner[...].astype(F32).T * values[...].astype(F32).T
    product[...] = mixed
    tail[...] = mixed[mixed.shape[0] - tail.shape[0] :, :]
    for copy in copies[:3] + copies[5:]:
        copy.wait()
    tokens, width = rows.shape
    capacity, columns = sent.shape[1:]
    wide = rows[...].astype(F32)
    scaling = lax.rsqrt(jnp.sum(wide * wide, axis=1, keepdims=True) / width + 1e-06)
    start = pl.multiple_of(place[0] * columns, columns)
    own = rows[:, pl.ds(start, columns)].astype(F32)
    normed = (own * scaling * gain[:, pl.ds(start, columns)]).astype(BF16)
    chosen = ids[...]
    expert = lax.broadcasted_iota(jnp.int32, (experts, tokens), 0)
    hits = [expert == chosen[k : k + 1, :] for k in range(chosen.shape[0])]
    marks = [jnp.where(h, 1.0, 0.0).astype(F32) for h in hits]
    total = marks[0]
    for m in marks[1:]:
        total = total + m
    earlier = lax.broadcasted_iota(jnp.int32, (tokens, tokens), 0)
    later = lax.broadcasted_iota(jnp.int32, (tokens, tokens), 1)
    before = jnp.dot(
        total.astype(BF16),
        jnp.where(earlier < later, 1.0, 0.0).astype(BF16),
        preferred_element_type=F32,
    )
    base = (expert * stride).astype(F32)
    where = [
        jnp.sum(m * (before + base), axis=0, keepdims=True).astype(jnp.int32) for m in marks
    ]
    slots[...] = jnp.concatenate(where, axis=0)
    slot = lax.broadcasted_iota(jnp.int32, (experts * stride, tokens), 0)
    table = slot == where[0]
    for w in where[1:]:
        table = table | (slot == w)
    placed = jnp.dot(
        jnp.where(table, 1.0, 0.0).astype(BF16), normed, preferred_element_type=F32
    ).reshape(experts, stride, columns)
    sent[...] = placed[:, :capacity, :].astype(BF16)


def weights_body(order, gate_far, up_far, down_far, gate_w, up_w, down_w, done):
    count = order.shape[0] // 2
    columns = gate_w.shape[0] // count
    copies = []
    for p in range(count):
        near = pl.ds(p * columns, columns)
        there = pl.ds(pl.multiple_of(order[p] * columns, columns), columns)
        for n, (source, target) in enumerate(
            (
                (gate_far.at[0, there, :], gate_w.at[near, :]),
                (up_far.at[0, there, :], up_w.at[near, :]),
                (down_far.at[0, :, there], down_w.at[:, near]),
            )
        ):
            copies.append(pltpu.make_async_copy(source, target, done.at[3 * p + n]))
            copies[-1].start()
    for copy in copies:
        copy.wait()


def expert_body(step, *refs):
    sides = (len(refs) - 3) // 2
    tokens, outs = refs[:sides], refs[sides + 3 :]
    gate_w, up_w, down_w = refs[sides : sides + 3]
    blocks, rows, columns = tokens[0].shape
    spots = [(n, m) for n in range(sides) for m in range(blocks)]

    def tile(number, carry):
        at = pl.ds(pl.multiple_of(number * step, step), step)
        left = jnp.concatenate([tokens[n][m, at, :] for n, m in spots], axis=1)
        gate = jnp.dot(left, gate_w[...], preferred_element_type=F32)
        up = jnp.dot(left, up_w[...], preferred_element_type=F32)
        hidden = (gate / (1.0 + jnp.exp(-gate)) * up).astype(BF16)
        part = jnp.dot(hidden, down_w[...], preferred_element_type=F32).astype(BF16)
        for p, (n, m) in enumerate(spots):
            outs[n][m, at, :] = part[:, p * columns : (p + 1) * columns]
        return carry

    lax.fori_loop(0, rows // step, tile, 0)


def fold_body(*refs):
    value = refs[0][...].astype(F32)
    for part in refs[1:-1]:
        value = value + part[...].astype(F32)
    refs[-1][...] = value.astype(BF16)


def sum_body(parts, out, total):
    experts, capacity, _ = out.shape
    value = parts[0].astype(F32)
    for b in range(1, parts.shape[0]):
        value = value + parts[b].astype(F32)
    total[...] = value
    for e in range(experts):
        out[e] = total[e * capacity : (e + 1) * capacity, :].astype(BF16)


def mixer_body(order, outer, product_ref, taps, halo, proj, *outs):
    groups, _, columns = outs[0].shape
    base = order.shape[0] // 2
    product = product_ref[...]
    row = lax.broadcasted_iota(jnp.int32, product.shape, 0)
    last = halo[1:2, :]
    back_one = jnp.where(row == 0, last, pltpu.roll(product, 1, 0))
    back_two = jnp.where(
        row == 0, halo[0:1, :], jnp.where(row == 1, last, pltpu.roll(product, 2, 0))
    )
    convolved = taps[0:1, :] * back_two + taps[1:2, :] * back_one + taps[2:3, :] * product
    branch = (outer[...].astype(F32).T * convolved).astype(BF16)
    for flip, out in enumerate(outs):
        for turn in range(groups):
            number = order[base + flip * groups + turn]
            start = pl.multiple_of(number * columns, columns)
            out[turn] = jnp.dot(
                branch, proj[:, pl.ds(start, columns)], preferred_element_type=F32
            ).astype(BF16)


def regroup_body(*refs):
    half = len(refs) // 2
    parts, outs = refs[:half], refs[half:]
    for turn, out in enumerate(outs):
        total = parts[0][turn].astype(F32)
        for part in parts[1:]:
            total = total + part[turn].astype(F32)
        out[...] = total.astype(BF16)


def final_body(*refs):
    total = refs[0][...].astype(F32)
    for part in refs[1:-1]:
        total = total + part[...].astype(F32)
    refs[-1][...] = total.astype(BF16)


PAIRS = (((1, 2), (3, 0)), ((0, 1), (2, 3)))


def squares(pairing):
    return [[(y, x) for y in ys for x in xs] for ys in PAIRS[pairing] for xs in PAIRS[pairing]]


def crossed(block, stage):
    names = ("ep",) + TP
    eps, _, xs = (lax.axis_size(name) for name in names)
    groups = []
    for e in range(eps):
        for square in squares((e + stage) % 2):
            groups.append([(e * xs + y) * xs + x for y, x in square])
    return lax.all_to_all(block, names, 0, 0, axis_index_groups=groups, tiled=True)


def flipped(spot, stage, flip):
    pair = {}
    for low, high in PAIRS[stage]:
        pair[low], pair[high] = high, low
    return (pair[spot[0]] if flip & 2 else spot[0], pair[spot[1]] if flip & 1 else spot[1])


def arrivals(side):
    rows = []
    for core in range(2):
        for y in range(side):
            for x in range(side):
                row = []
                for flip in range(4):
                    member = flipped((y, x), (core + 1) % 2, flip)
                    group = next(g for g in squares(core % 2) if member in g)
                    row += [there_y * side + there_x for there_y, there_x in group]
                for flip in range(4):
                    member = flipped((y, x), (core + 1) % 2, flip)
                    for turn in range(4):
                        there_y, there_x = flipped(member, core, turn)
                        row.append(there_y * side + there_x)
                rows.append(row)
    return rows


def swapped(block, flip, stage=1):
    names = ("ep",) + TP
    eps, ys, xs = (lax.axis_size(name) for name in names)
    route = []
    for e in range(eps):
        for y in range(ys):
            for x in range(xs):
                to_y, to_x = flipped((y, x), (e + stage) % 2, flip)
                route.append(((e * ys + y) * xs + x, (e * ys + to_y) * xs + to_x))
    return lax.ppermute(block, names, route)


def combine_body(rows, slots, scores, out, padded):
    tokens = out.shape[0]
    experts, capacity, columns = rows.shape
    stride = padded.shape[1]
    slot = lax.broadcasted_iota(jnp.int32, (tokens, experts * stride), 1)
    padded[...] = jnp.zeros_like(padded)
    padded[:, :capacity, :] = rows[...].astype(F32)
    held = padded[...].reshape(experts * stride, columns).astype(BF16)
    score = scores[...]
    whole = jnp.sum(score, axis=1, keepdims=True)
    total = None
    for k in range(score.shape[1]):
        pick = jnp.where(slot == slots[:, k : k + 1], 1.0, 0.0).astype(BF16)
        term = jnp.dot(pick, held, preferred_element_type=F32)
        term = term * (score[:, k : k + 1] / whole)
        total = term if total is None else total + term
    out[...] = total.astype(BF16)


def shards(
    gate_out,
    gate_in,
    conv_values,
    conv_taps,
    mixer_proj,
    expert_in,
    norm_gain,
    route_ids,
    route_scores,
    gate_proj,
    up_proj,
    down_proj,
):
    tokens, choices = route_ids.shape
    width = expert_in.shape[1]
    ep_count = lax.axis_size("ep")
    tp_count = lax.axis_size(TP)
    local_experts = gate_proj.shape[0]
    experts = ep_count * local_experts
    capacity = max(2, (4 * tokens * choices + 3 * experts - 1) // (3 * experts))
    slot_count = experts * capacity
    stride = (capacity + 7) // 8 * 8
    columns = width // tp_count
    place = lax.axis_index(TP).astype(jnp.int32).reshape(1)
    side = lax.axis_size(TP[0])
    table = jnp.array(arrivals(side), jnp.int32)
    order = lax.dynamic_index_in_dim(
        table, (lax.axis_index("ep") % 2) * tp_count + lax.axis_index(TP), keepdims=False
    )
    groups = lax.axis_size(TP[0])
    turns = lax.axis_size(TP[1])
    seq_len = gate_in.shape[0]
    channels = gate_in.shape[1]

    sent, slots, tail, product, outer, proj, taps = call(
        lambda *refs: dispatch_body(stride, experts, *refs),
        (
            jax.ShapeDtypeStruct((experts, capacity, columns), BF16),
            jax.ShapeDtypeStruct((choices, tokens), jnp.int32),
            jax.ShapeDtypeStruct((conv_taps.shape[0] - 1, channels), F32),
            jax.ShapeDtypeStruct((seq_len, channels), F32),
            jax.ShapeDtypeStruct((channels, seq_len), BF16),
            jax.ShapeDtypeStruct(mixer_proj.shape, BF16),
            jax.ShapeDtypeStruct(conv_taps.shape, F32),
        ),
        16 << 20,
        1 << 28,
        place,
        far(expert_in),
        far(norm_gain.reshape(1, width)),
        far(route_ids.T),
        far(gate_in.T),
        far(conv_values.T),
        far(gate_out.T),
        far(mixer_proj),
        far(conv_taps),
        specs=[SMEM] + [HBM] * 8,
        scratch=[
            pltpu.VMEM((tokens, width), BF16),
            pltpu.VMEM((1, width), F32),
            pltpu.VMEM((choices, tokens), jnp.int32),
            pltpu.VMEM((channels, seq_len), BF16),
            pltpu.VMEM((channels, seq_len), BF16),
            pltpu.SemaphoreType.DMA((8,)),
        ],
    )
    halo = shifted(tail, "ep", 1)
    arrived = lax.all_to_all(sent, "ep", 0, 0, tiled=True)

    first = call(
        mixer_body,
        (jax.ShapeDtypeStruct((groups, seq_len, columns), BF16),) * turns,
        12 << 20,
        1 << 26,
        order,
        outer,
        product,
        taps,
        halo,
        proj,
        specs=[SMEM] + [VMEM] * 5,
    )
    first = list(first)
    for flip in (1, 2, 3):
        first[flip] = swapped(first[flip], flip)

    block = (slot_count, columns)
    own_block = jnp.broadcast_to(arrived.reshape(1, *block), (side, *block))
    own_block, order = lax.optimization_barrier((own_block, order))
    line = crossed(own_block, 0)
    lines = [line]
    for flip in (1, 2, 3):
        lines.append(swapped(line, flip))
    weights = call(
        weights_body,
        tuple(
            jax.ShapeDtypeStruct(w.shape[1:], BF16) for w in (gate_proj, up_proj, down_proj)
        ),
        8 << 20,
        1 << 22,
        order,
        far(gate_proj),
        far(up_proj),
        far(down_proj),
        specs=[SMEM, HBM, HBM, HBM],
        scratch=[pltpu.SemaphoreType.DMA((3 * tp_count,))],
    )
    parts = call(
        lambda *refs: expert_body(slot_count, *refs),
        (jax.ShapeDtypeStruct((side, *block), BF16),) * side,
        24 << 20,
        1 << 32,
        *lines,
        *weights,
    )
    parts = list(parts)
    for flip in (1, 2, 3):
        parts[flip] = swapped(parts[flip], flip)
    line = call(
        fold_body,
        jax.ShapeDtypeStruct((side, *block), BF16),
        16 << 20,
        1 << 24,
        *parts,
    )
    shared = crossed(line, 0)
    outputs = call(
        sum_body,
        jax.ShapeDtypeStruct((experts, capacity, columns), BF16),
        16 << 20,
        1 << 24,
        shared,
        scratch=[pltpu.VMEM((slot_count, columns), F32)],
    )
    returned = lax.all_to_all(outputs, "ep", 0, 0, tiled=True)

    second = call(
        regroup_body,
        (jax.ShapeDtypeStruct((seq_len, columns), BF16),) * groups,
        12 << 20,
        1 << 22,
        *first,
    )
    second = list(second)
    for flip in (1, 2, 3):
        second[flip] = swapped(second[flip], flip, 0)
    mixed = call(
        final_body, jax.ShapeDtypeStruct((seq_len, columns), BF16), 8 << 20, 1 << 20, *second
    )
    expert_mix = call(
        combine_body,
        jax.ShapeDtypeStruct((tokens, columns), BF16),
        16 << 20,
        1 << 27,
        returned,
        slots.T,
        route_scores,
        scratch=[pltpu.VMEM((experts, stride, columns), F32)],
    )
    return (mixed, expert_mix)


def solution(mesh):
    torus = Mesh(mesh.devices.reshape(mesh.shape["ep"], 4, 4), ("ep", "tp_0", "tp_1"))
    in_specs = (
        P("ep", TP),
        P("ep", TP),
        P("ep", TP),
        P(None, TP),
        P(TP, None),
        P("ep", None),
        P(),
        P("ep", None),
        P("ep", None),
        P("ep", None, TP),
        P("ep", None, TP),
        P("ep", TP, None),
    )
    out_specs = (P("ep", TP), P("ep", TP))

    return jax.shard_map(
        shards, mesh=torus, in_specs=in_specs, out_specs=out_specs, check_vma=False
    )
```

```python
import jax
import jax.numpy as jnp
from jax import lax
from jax.experimental import pallas as pl
from jax.experimental.pallas import tpu as pltpu
from jax.sharding import Mesh
from jax.sharding import PartitionSpec as P


TP = ("tp_0", "tp_1")
F32 = jnp.float32
BF16 = jnp.bfloat16
VMEM = pl.BlockSpec(memory_space=pltpu.VMEM)
SMEM = pl.BlockSpec(memory_space=pltpu.SMEM)
HBM = pl.BlockSpec(memory_space=pltpu.HBM)


def shifted(block, axis, distance):
    devices = range(lax.axis_size(axis))
    route = [(i - distance, i) for i in devices if i - distance in devices]
    return lax.ppermute(block, axis, route)


def call(body, out, limit, flops, *operands, specs=None, scratch=(), place=None):
    return pl.pallas_call(
        body,
        out_shape=out,
        in_specs=specs or [VMEM] * len(operands),
        out_specs=jax.tree.map(lambda _: place or VMEM, out),
        scratch_shapes=scratch,
        compiler_params=pltpu.CompilerParams(vmem_limit_bytes=limit),
        cost_estimate=pl.CostEstimate(
            flops=flops, bytes_accessed=1 << 20, transcendentals=0
        ),
    )(*operands)


def far(array):
    return pltpu.with_memory_space_constraint(array, pltpu.HBM)


def dispatch_body(
    stride,
    experts,
    place,
    rows_far,
    gain_far,
    ids_far,
    inner_far,
    values_far,
    outer_far,
    proj_far,
    taps_far,
    sent,
    slots,
    tail,
    product,
    outer,
    proj,
    taps,
    rows,
    gain,
    ids,
    inner,
    values,
    done,
):
    pairs = (
        (rows_far, rows),
        (gain_far, gain),
        (ids_far, ids),
        (inner_far, inner),
        (values_far, values),
        (outer_far, outer),
        (proj_far, proj),
        (taps_far, taps),
    )
    copies = [
        pltpu.make_async_copy(there, here, done.at[n]) for n, (there, here) in enumerate(pairs)
    ]
    for copy in copies:
        copy.start()
    for copy in copies[3:5]:
        copy.wait()
    mixed = inner[...].astype(F32).T * values[...].astype(F32).T
    product[...] = mixed
    tail[...] = mixed[mixed.shape[0] - tail.shape[0] :, :]
    for copy in copies[:3] + copies[5:]:
        copy.wait()
    tokens, width = rows.shape
    capacity, columns = sent.shape[1:]
    wide = rows[...].astype(F32)
    scaling = lax.rsqrt(jnp.sum(wide * wide, axis=1, keepdims=True) / width + 1e-06)
    start = pl.multiple_of(place[0] * columns, columns)
    own = rows[:, pl.ds(start, columns)].astype(F32)
    normed = (own * scaling * gain[:, pl.ds(start, columns)]).astype(BF16)
    chosen = ids[...]
    expert = lax.broadcasted_iota(jnp.int32, (experts, tokens), 0)
    hits = [expert == chosen[k : k + 1, :] for k in range(chosen.shape[0])]
    marks = [jnp.where(h, 1.0, 0.0).astype(F32) for h in hits]
    total = marks[0]
    for m in marks[1:]:
        total = total + m
    earlier = lax.broadcasted_iota(jnp.int32, (tokens, tokens), 0)
    later = lax.broadcasted_iota(jnp.int32, (tokens, tokens), 1)
    before = jnp.dot(
        total.astype(BF16),
        jnp.where(earlier < later, 1.0, 0.0).astype(BF16),
        preferred_element_type=F32,
    )
    base = (expert * stride).astype(F32)
    where = [
        jnp.sum(m * (before + base), axis=0, keepdims=True).astype(jnp.int32) for m in marks
    ]
    slots[...] = jnp.concatenate(where, axis=0)
    slot = lax.broadcasted_iota(jnp.int32, (experts * stride, tokens), 0)
    table = slot == where[0]
    for w in where[1:]:
        table = table | (slot == w)
    placed = jnp.dot(
        jnp.where(table, 1.0, 0.0).astype(BF16), normed, preferred_element_type=F32
    ).reshape(experts, stride, columns)
    sent[...] = placed[:, :capacity, :].astype(BF16)


def weights_body(order, gate_far, up_far, down_far, gate_w, up_w, down_w, done):
    count = order.shape[0] // 2
    columns = gate_w.shape[0] // count
    copies = []
    for p in range(count):
        near = pl.ds(p * columns, columns)
        there = pl.ds(pl.multiple_of(order[p] * columns, columns), columns)
        for n, (source, target) in enumerate(
            (
                (gate_far.at[0, there, :], gate_w.at[near, :]),
                (up_far.at[0, there, :], up_w.at[near, :]),
                (down_far.at[0, :, there], down_w.at[:, near]),
            )
        ):
            copies.append(pltpu.make_async_copy(source, target, done.at[3 * p + n]))
            copies[-1].start()
    for copy in copies:
        copy.wait()


def expert_body(*refs):
    sides = len(refs) - 6
    tokens = refs[:sides]
    gate_w, up_w, down_w, hidden_out = refs[sides : sides + 4]
    outs = refs[sides + 4 :]
    blocks, _, columns = tokens[0].shape
    left = jnp.concatenate([t[m] for t in tokens for m in range(blocks)], axis=1)
    gate = jnp.dot(left, gate_w[...], preferred_element_type=F32)
    up = jnp.dot(left, up_w[...], preferred_element_type=F32)
    hidden = (gate / (1.0 + jnp.exp(-gate)) * up).astype(BF16)
    hidden_out[...] = hidden
    first = (sides - len(outs)) * blocks * columns
    part = jnp.dot(hidden, down_w[:, first:], preferred_element_type=F32).astype(BF16)
    for p in range(len(outs) * blocks):
        outs[p // blocks][p % blocks] = part[:, p * columns : (p + 1) * columns]


def rest_body(hidden, down_w, *outs):
    blocks, _, columns = outs[0].shape
    width = len(outs) * blocks * columns
    part = jnp.dot(hidden[...], down_w[:, :width], preferred_element_type=F32).astype(BF16)
    for p in range(len(outs) * blocks):
        outs[p // blocks][p % blocks] = part[:, p * columns : (p + 1) * columns]


def fold_body(*refs):
    value = refs[0][...].astype(F32)
    for part in refs[1:-1]:
        value = value + part[...].astype(F32)
    refs[-1][...] = value.astype(BF16)


def sum_body(parts, out, total):
    experts, capacity, _ = out.shape
    value = parts[0].astype(F32)
    for b in range(1, parts.shape[0]):
        value = value + parts[b].astype(F32)
    total[...] = value
    for e in range(experts):
        out[e] = total[e * capacity : (e + 1) * capacity, :].astype(BF16)


def mixer_body(order, outer, product_ref, taps, halo, proj, *outs):
    groups, _, columns = outs[0].shape
    base = order.shape[0] // 2
    product = product_ref[...]
    row = lax.broadcasted_iota(jnp.int32, product.shape, 0)
    last = halo[1:2, :]
    back_one = jnp.where(row == 0, last, pltpu.roll(product, 1, 0))
    back_two = jnp.where(
        row == 0, halo[0:1, :], jnp.where(row == 1, last, pltpu.roll(product, 2, 0))
    )
    convolved = taps[0:1, :] * back_two + taps[1:2, :] * back_one + taps[2:3, :] * product
    branch = (outer[...].astype(F32).T * convolved).astype(BF16)
    for flip, out in enumerate(outs):
        for turn in range(groups):
            number = order[base + flip * groups + turn]
            start = pl.multiple_of(number * columns, columns)
            out[turn] = jnp.dot(
                branch, proj[:, pl.ds(start, columns)], preferred_element_type=F32
            ).astype(BF16)


def regroup_body(*refs):
    half = len(refs) // 2
    parts, outs = refs[:half], refs[half:]
    for turn, out in enumerate(outs):
        total = parts[0][turn].astype(F32)
        for part in parts[1:]:
            total = total + part[turn].astype(F32)
        out[...] = total.astype(BF16)


def final_body(*refs):
    total = refs[0][...].astype(F32)
    for part in refs[1:-1]:
        total = total + part[...].astype(F32)
    refs[-1][...] = total.astype(BF16)


PAIRS = (((1, 2), (3, 0)), ((0, 1), (2, 3)))


def squares(pairing):
    return [[(y, x) for y in ys for x in xs] for ys in PAIRS[pairing] for xs in PAIRS[pairing]]


def crossed(block, stage):
    names = ("ep",) + TP
    eps, _, xs = (lax.axis_size(name) for name in names)
    groups = []
    for e in range(eps):
        for square in squares((e + stage) % 2):
            groups.append([(e * xs + y) * xs + x for y, x in square])
    return lax.all_to_all(block, names, 0, 0, axis_index_groups=groups, tiled=True)


def flipped(spot, stage, flip):
    pair = {}
    for low, high in PAIRS[stage]:
        pair[low], pair[high] = high, low
    return (pair[spot[0]] if flip & 2 else spot[0], pair[spot[1]] if flip & 1 else spot[1])


def arrivals(side):
    rows = []
    for core in range(2):
        for y in range(side):
            for x in range(side):
                row = []
                for flip in range(4):
                    member = flipped((y, x), (core + 1) % 2, flip)
                    group = next(g for g in squares(core % 2) if member in g)
                    row += [there_y * side + there_x for there_y, there_x in group]
                for flip in range(4):
                    member = flipped((y, x), (core + 1) % 2, flip)
                    for turn in range(4):
                        there_y, there_x = flipped(member, core, turn)
                        row.append(there_y * side + there_x)
                rows.append(row)
    return rows


def swapped(block, flip, stage=1):
    names = ("ep",) + TP
    eps, ys, xs = (lax.axis_size(name) for name in names)
    route = []
    for e in range(eps):
        for y in range(ys):
            for x in range(xs):
                to_y, to_x = flipped((y, x), (e + stage) % 2, flip)
                route.append(((e * ys + y) * xs + x, (e * ys + to_y) * xs + to_x))
    return lax.ppermute(block, names, route)


def combine_body(rows, slots, scores, out, padded):
    tokens = out.shape[0]
    experts, capacity, columns = rows.shape
    stride = padded.shape[1]
    slot = lax.broadcasted_iota(jnp.int32, (tokens, experts * stride), 1)
    padded[...] = jnp.zeros_like(padded)
    padded[:, :capacity, :] = rows[...].astype(F32)
    held = padded[...].reshape(experts * stride, columns).astype(BF16)
    score = scores[...]
    whole = jnp.sum(score, axis=1, keepdims=True)
    total = None
    for k in range(score.shape[1]):
        pick = jnp.where(slot == slots[:, k : k + 1], 1.0, 0.0).astype(BF16)
        term = jnp.dot(pick, held, preferred_element_type=F32)
        term = term * (score[:, k : k + 1] / whole)
        total = term if total is None else total + term
    out[...] = total.astype(BF16)


def shards(
    gate_out,
    gate_in,
    conv_values,
    conv_taps,
    mixer_proj,
    expert_in,
    norm_gain,
    route_ids,
    route_scores,
    gate_proj,
    up_proj,
    down_proj,
):
    tokens, choices = route_ids.shape
    width = expert_in.shape[1]
    ep_count = lax.axis_size("ep")
    tp_count = lax.axis_size(TP)
    local_experts = gate_proj.shape[0]
    experts = ep_count * local_experts
    capacity = max(2, (4 * tokens * choices + 3 * experts - 1) // (3 * experts))
    slot_count = experts * capacity
    stride = (capacity + 7) // 8 * 8
    columns = width // tp_count
    place = lax.axis_index(TP).astype(jnp.int32).reshape(1)
    side = lax.axis_size(TP[0])
    table = jnp.array(arrivals(side), jnp.int32)
    order = lax.dynamic_index_in_dim(
        table, (lax.axis_index("ep") % 2) * tp_count + lax.axis_index(TP), keepdims=False
    )
    groups = lax.axis_size(TP[0])
    turns = lax.axis_size(TP[1])
    seq_len = gate_in.shape[0]
    channels = gate_in.shape[1]

    sent, slots, tail, product, outer, proj, taps = call(
        lambda *refs: dispatch_body(stride, experts, *refs),
        (
            jax.ShapeDtypeStruct((experts, capacity, columns), BF16),
            jax.ShapeDtypeStruct((choices, tokens), jnp.int32),
            jax.ShapeDtypeStruct((conv_taps.shape[0] - 1, channels), F32),
            jax.ShapeDtypeStruct((seq_len, channels), F32),
            jax.ShapeDtypeStruct((channels, seq_len), BF16),
            jax.ShapeDtypeStruct(mixer_proj.shape, BF16),
            jax.ShapeDtypeStruct(conv_taps.shape, F32),
        ),
        16 << 20,
        1 << 28,
        place,
        far(expert_in),
        far(norm_gain.reshape(1, width)),
        far(route_ids.T),
        far(gate_in.T),
        far(conv_values.T),
        far(gate_out.T),
        far(mixer_proj),
        far(conv_taps),
        specs=[SMEM] + [HBM] * 8,
        scratch=[
            pltpu.VMEM((tokens, width), BF16),
            pltpu.VMEM((1, width), F32),
            pltpu.VMEM((choices, tokens), jnp.int32),
            pltpu.VMEM((channels, seq_len), BF16),
            pltpu.VMEM((channels, seq_len), BF16),
            pltpu.SemaphoreType.DMA((8,)),
        ],
    )
    halo = shifted(tail, "ep", 1)
    arrived = lax.all_to_all(sent, "ep", 0, 0, tiled=True)

    first = call(
        mixer_body,
        (jax.ShapeDtypeStruct((groups, seq_len, columns), BF16),) * turns,
        12 << 20,
        1 << 26,
        order,
        outer,
        product,
        taps,
        halo,
        proj,
        specs=[SMEM] + [VMEM] * 5,
    )
    first = list(first)
    for flip in (1, 2, 3):
        first[flip] = swapped(first[flip], flip)

    block = (slot_count, columns)
    own_block = jnp.broadcast_to(arrived.reshape(1, *block), (side, *block))
    own_block, order = lax.optimization_barrier((own_block, order))
    line = crossed(own_block, 0)
    lines = [line]
    for flip in (1, 2, 3):
        lines.append(swapped(line, flip))
    weights = call(
        weights_body,
        tuple(
            jax.ShapeDtypeStruct(w.shape[1:], BF16) for w in (gate_proj, up_proj, down_proj)
        ),
        8 << 20,
        1 << 22,
        order,
        far(gate_proj),
        far(up_proj),
        far(down_proj),
        specs=[SMEM, HBM, HBM, HBM],
        scratch=[pltpu.SemaphoreType.DMA((3 * tp_count,))],
    )
    hidden, *last = call(
        expert_body,
        (jax.ShapeDtypeStruct((slot_count, gate_proj.shape[2]), BF16),)
        + (jax.ShapeDtypeStruct((side, *block), BF16),) * 2,
        24 << 20,
        1 << 31,
        *lines,
        *weights,
    )
    parts = call(
        rest_body,
        (jax.ShapeDtypeStruct((side, *block), BF16),) * 2,
        24 << 20,
        1 << 29,
        hidden,
        weights[2],
    )
    parts = list(parts) + list(last)
    for flip in (1, 2, 3):
        parts[flip] = swapped(parts[flip], flip)
    line = call(
        fold_body,
        jax.ShapeDtypeStruct((side, *block), BF16),
        16 << 20,
        1 << 24,
        *parts,
    )
    shared = crossed(line, 0)
    outputs = call(
        sum_body,
        jax.ShapeDtypeStruct((experts, capacity, columns), BF16),
        16 << 20,
        1 << 24,
        shared,
        scratch=[pltpu.VMEM((slot_count, columns), F32)],
    )
    returned = lax.all_to_all(outputs, "ep", 0, 0, tiled=True)

    second = call(
        regroup_body,
        (jax.ShapeDtypeStruct((seq_len, columns), BF16),) * groups,
        12 << 20,
        1 << 22,
        *first,
    )
    second = list(second)
    for flip in (1, 2, 3):
        second[flip] = swapped(second[flip], flip, 0)
    mixed = call(
        final_body, jax.ShapeDtypeStruct((seq_len, columns), BF16), 8 << 20, 1 << 20, *second
    )
    expert_mix = call(
        combine_body,
        jax.ShapeDtypeStruct((tokens, columns), BF16),
        16 << 20,
        1 << 27,
        returned,
        slots.T,
        route_scores,
        scratch=[pltpu.VMEM((experts, stride, columns), F32)],
    )
    return (mixed, expert_mix)


def solution(mesh):
    torus = Mesh(mesh.devices.reshape(mesh.shape["ep"], 4, 4), ("ep", "tp_0", "tp_1"))
    in_specs = (
        P("ep", TP),
        P("ep", TP),
        P("ep", TP),
        P(None, TP),
        P(TP, None),
        P("ep", None),
        P(),
        P("ep", None),
        P("ep", None),
        P("ep", None, TP),
        P("ep", None, TP),
        P("ep", TP, None),
    )
    out_specs = (P("ep", TP), P("ep", TP))

    return jax.shard_map(
        shards, mesh=torus, in_specs=in_specs, out_specs=out_specs, check_vma=False
    )
```
